32 devices in a mesh: sp: 4 (over y, x), tp: 8 (over z, core).
Axes of the slice: x: 2, y: 2, z: 4, core: 2. Of those that a mesh axis runs over, the one named last changes fastest.
Arguments:
- residual: bfloat16 [1536, 2048], P(('sp', 'tp')), may hold values from -40 to 40
- queries: bfloat16 [1536, 16, 256], P('sp', 'tp'), may hold values from -8.8 to 8.8
- query_rope: bfloat16 [1536, 16, 64], P('sp', 'tp'), may hold values from -72 to 72
- latent: bfloat16 [1536, 512], P('sp'), may hold values from -320 to 320
- key_rope: bfloat16 [1536, 32], P('sp'), may hold values from -48 to 48
- latent_gain: float32 [512], replicated, may hold values from 0.1 to 1.9
- key_weight: bfloat16 [512, 16, 256], P(None, 'tp'), may hold values from -0.25 to 0.25
- value_weight: bfloat16 [512, 16, 256], P(None, 'tp'), may hold values from -0.25 to 0.25
- out_weight: bfloat16 [16, 256, 2048], P('tp'), may hold values from -0.09375 to 0.09375
- norm_gain: float32 [2048], replicated, may hold values from 0.1 to 1.9
- routes: int32 [1536, 2], P('sp'), may hold values from 0 to 7, as said below
- group_gate: float32 [1536], P(('sp', 'tp')), may hold values from 0.5 to 1
- expert_share: float32 [1536, 2], P(('sp', 'tp')), may hold values from 0.2 to 1
- gate_weight: bfloat16 [8, 2048, 4096], P('sp', None, 'tp'), may hold values from -0.125 to 0.125
- up_weight: bfloat16 [8, 2048, 4096], P('sp', None, 'tp'), may hold values from -0.125 to 0.125
- down_weight: bfloat16 [8, 4096, 2048], P('sp', 'tp'), may hold values from -0.1875 to 0.1875
Outputs:
- layer_out: bfloat16 [1536, 2048], P(('sp', 'tp'))
The draws below stay inside these ranges and needn't reach their ends.
Inputs may be any that keep to these rules, and one draw needn't show every extreme that they name: `routes`: each token names two different experts of one group; expert e belongs to group e // 2. In each aligned block of 48 tokens no expert is named more than 18 times, and one expert, the same in every block, is named exactly 18 times in every block.
All inputs are finite; a program needn't handle non-finite values.
Results may differ from the reference program's by a relative error of at most 0.025.
Values may be sent and summed in bfloat16 or wider, within the bound.
A program may use at most 64 MiB of HBM per device.

```python
import math
import jax
import jax.numpy as jnp
from jax import lax

D = 2048
PAIRS = 16
DK_A = 64
DV_A = 64
DK_B = 192
DV_B = 192
DR = 32
LATENT = 512
FF = 4096
GROUPS = 4
TOPK = 2
SEQ = 1536
PAIR_DEV = 2
ROWS = 48
FF_DEV = 512
EXPERTS = 8
CAP = 18
N_TP = 8


def rough_field(key, salt_value, columns):
    values = jnp.clip(jax.random.normal(jax.random.fold_in(key, salt_value), (SEQ, columns), jnp.float32), -4.0, 4.0)
    return values


def draw_residual(key, part):
    return (0.25 * rough_field(key, 40, D)).astype(jnp.bfloat16)


def draw_latent(key, part):
    return rough_field(key, 50, LATENT).astype(jnp.bfloat16)


def draw_queries(key, part):
    own_key = jax.random.fold_in(key, 23)
    array_shape = (SEQ, PAIRS, DK_A + DK_B)
    return jnp.clip(2.2 * jax.random.normal(own_key, array_shape, jnp.float32), -8.75, 8.75).astype(jnp.bfloat16)


def draw_query_rope(key, part):
    own_key = jax.random.fold_in(key, 21)
    array_shape = (SEQ, PAIRS, 2 * DR)
    return jnp.clip(2.2 * jax.random.normal(own_key, array_shape, jnp.float32), -8.75, 8.75).astype(jnp.bfloat16)


def draw_key_rope(key, part):
    own_key = jax.random.fold_in(key, 22)
    base_values = jnp.clip(jax.random.normal(own_key, (SEQ, DR), jnp.float32), -4.0, 4.0)
    return base_values.astype(jnp.bfloat16)


def draw_routes(key, part):
    blocks = SEQ // ROWS
    within = EXPERTS // GROUPS
    pair_total = EXPERTS // 2
    hot_rows = 0
    while hot_rows + (ROWS - hot_rows + pair_total - 1) // pair_total != CAP:
        hot_rows += 1
    key_list = jax.random.split(jax.random.fold_in(key, 31), 5)
    favored = jax.random.randint(key_list[0], (), 0, EXPERTS, dtype=jnp.int32)
    favored_group = favored // within
    favored_place = favored % within
    member = jnp.arange(within, dtype=jnp.int32)
    ranking = jax.random.randint(key_list[1], (blocks, GROUPS, within), 0, 1 << 20, dtype=jnp.int32) * within + member
    place_order = jnp.argsort(ranking, axis=2).astype(jnp.int32)
    leading = place_order[:, :, :1]
    swapped = jnp.where(place_order == favored_place, leading, place_order)
    swapped = jnp.where(member[None, None, :] == 0, favored_place, swapped)
    is_favored = (jnp.arange(GROUPS, dtype=jnp.int32) == favored_group)[None, :, None]
    place_order = jnp.where(is_favored, swapped, place_order)
    expert_table = place_order + (jnp.arange(GROUPS, dtype=jnp.int32) * within)[None, :, None]
    pair_table = expert_table.reshape(blocks, pair_total, 2)
    pair_ids = jnp.arange(pair_total, dtype=jnp.int32)
    pair_rank = jax.random.randint(key_list[2], (blocks, pair_total), 0, 1 << 20, dtype=jnp.int32) * pair_total + pair_ids
    pair_rank = jnp.where(pair_ids[None, :] == favored_group * (within // 2), -1, pair_rank)
    pair_order = jnp.argsort(pair_rank, axis=1)
    pair_table = jnp.take_along_axis(pair_table, pair_order[:, :, None], axis=1)
    row_ids = jnp.arange(ROWS, dtype=jnp.int32)
    cycled = jnp.take(pair_table, (row_ids - hot_rows) % pair_total, axis=1)
    favored_row = jnp.take(expert_table, favored_group, axis=1)
    partner = jnp.take(favored_row, 1 + row_ids % (within - 1), axis=1)
    hot_pair = jnp.stack([jnp.broadcast_to(favored, partner.shape), partner], axis=2)
    chosen = jnp.where((row_ids < hot_rows)[None, :, None], hot_pair, cycled)
    flip_bits = jax.random.randint(key_list[3], (blocks, ROWS, 1), 0, 2, dtype=jnp.int32)
    chosen = jnp.where(flip_bits == 1, chosen[:, :, ::-1], chosen)
    shuffle = jnp.argsort(jax.random.randint(key_list[4], (blocks, ROWS), 0, 1 << 20, dtype=jnp.int32) * ROWS + row_ids[None, :], axis=1)
    chosen = jnp.take_along_axis(chosen, shuffle[:, :, None], axis=1)
    return chosen.reshape(SEQ, 2).astype(jnp.int32)


def block_levels(rng, shape, pieces, smallest, top_value):
    def one(axis_at, parts):
        steps = jax.random.uniform(jax.random.fold_in(jax.random.fold_in(rng, 6), axis_at), (parts,), jnp.float32, smallest / len(pieces), top_value / len(pieces))
        return jnp.repeat(jnp.exp(steps), shape[axis_at] // parts).reshape((-1,) + (1,) * (len(shape) - axis_at - 1))

    level = one(*pieces[0])
    for cut in pieces[1:]:
        level = level * one(*cut)
    return level


def scatter_about(key, shape, deviation, limit, cuts=(), kind=jnp.bfloat16):
    array = jax.random.normal(key, shape, jnp.float32) * deviation
    if len(cuts) > 0:
        array = block_levels(key, shape, cuts, -0.22, 0.18) * array
    return jnp.clip(array, min=-limit, max=limit).astype(kind)


def setup_inputs(seed: int = 0) -> dict:
    splits = jax.random.split(jax.random.key(seed), 17)
    residual = draw_residual(jax.random.fold_in(splits[16], 71), 0)
    queries = draw_queries(jax.random.fold_in(splits[16], 71), 0)
    query_rope = draw_query_rope(jax.random.fold_in(splits[16], 71), 0)
    latent = draw_latent(jax.random.fold_in(splits[16], 71), 0)
    key_rope = draw_key_rope(jax.random.fold_in(splits[16], 71), 0)
    latent_gain = jnp.clip(1.0 + 0.18 * jax.random.normal(splits[5], (LATENT,), jnp.float32), 0.1, 1.9)
    key_weight = scatter_about(splits[6], (LATENT, PAIRS, DK_A + DK_B), LATENT ** -0.5, 0.25, ((1, 8),))
    value_weight = scatter_about(splits[7], (LATENT, PAIRS, DV_A + DV_B), LATENT ** -0.5, 0.25, ((1, 8),))
    out_weight = scatter_about(splits[8], (PAIRS, DV_A + DV_B, D), (PAIRS * (DV_A + DV_B)) ** -0.5, 0.09375, ((0, 8),))
    norm_gain = jnp.clip(1.0 + 0.18 * jax.random.normal(splits[9], (D,), jnp.float32), 0.1, 1.9)
    routes = draw_routes(jax.random.fold_in(splits[16], 71), 0)
    group_gate = jnp.clip(jnp.exp(math.log(1.0) - 0.6931472 * jax.random.uniform(splits[11], (SEQ,), jnp.float32) ** block_levels(splits[11], (SEQ,), ((0, 32),), -0.2, 0.2)), 0.5, 1.0)
    expert_share = jnp.clip(jnp.exp(math.log(1.0) - 1.609438 * jax.random.uniform(splits[12], (SEQ, TOPK), jnp.float32) ** block_levels(splits[12], (SEQ, TOPK), ((0, 32),), -0.2, 0.2)), 0.2, 1.0)
    gate_weight = scatter_about(splits[13], (EXPERTS, D, FF), D ** -0.5, 0.125, ((0, 4), (2, 8)))
    up_weight = scatter_about(splits[14], (EXPERTS, D, FF), D ** -0.5, 0.125, ((0, 4), (2, 8)))
    down_weight = scatter_about(splits[15], (EXPERTS, FF, D), (FF // 4) ** -0.5, 0.1875, ((0, 4), (1, 8)))
    return {"residual": residual, "queries": queries, "query_rope": query_rope, "latent": latent, "key_rope": key_rope, "latent_gain": latent_gain, "key_weight": key_weight, "value_weight": value_weight, "out_weight": out_weight, "norm_gain": norm_gain, "routes": routes, "group_gate": group_gate, "expert_share": expert_share, "gate_weight": gate_weight, "up_weight": up_weight, "down_weight": down_weight}


rope_base = 10000.0
epsilon = 1e-06

def angle_tables(places, rope_width):
    frequencies = rope_base ** (-jnp.arange(0, rope_width, 2, dtype=jnp.float32) / rope_width)
    angles = places[:, None] * frequencies[None, :]
    return (jnp.cos(angles), jnp.sin(angles))

def rope_turn(values, cosine, sine_table):
    half_size = values.shape[-1] // 2
    first_half = values[..., :half_size]
    second = values[..., half_size:]
    return jnp.concatenate([first_half * cosine - second * sine_table, second * cosine + first_half * sine_table], axis=-1)

def rms_scale(values, gain_vector):
    values = values.astype(jnp.float32)
    inverse = lax.rsqrt(lax.optimization_barrier(jnp.mean(values * values, axis=-1, keepdims=True)) + epsilon)
    return values * inverse * gain_vector.astype(jnp.float32)

def group_attend(query_nope, query_turned, key_nope, rotated_key, value_part, visible, scale):
    scores = jnp.einsum('qhd,khd->hqk', query_nope.astype(jnp.float32), key_nope.astype(jnp.float32))
    scores = scores + jnp.einsum('qhd,kd->hqk', query_turned.astype(jnp.float32), rotated_key.astype(jnp.float32))
    scores = scores * scale
    masked = jnp.where(visible[None], scores, -jnp.inf)
    row_top = lax.optimization_barrier(jnp.max(masked, axis=2, keepdims=True))
    weights = jnp.exp(masked - row_top)
    weight_sum = lax.optimization_barrier(jnp.sum(weights, axis=2))
    rounded = lax.optimization_barrier(weights.astype(jnp.bfloat16)).astype(jnp.float32)
    mixed_rows = jnp.einsum('hqk,khd->qhd', rounded, value_part.astype(jnp.float32))
    return (mixed_rows / jnp.transpose(weight_sum)[:, :, None]).astype(jnp.bfloat16)

def reference(residual, queries, query_rope, latent, key_rope, latent_gain, key_weight, value_weight, out_weight, norm_gain, routes, group_gate, expert_share, gate_weight, up_weight, down_weight):
    places = jnp.arange(SEQ, dtype=jnp.int32).astype(jnp.float32)
    cosine, sine_table = angle_tables(places, DR)
    compressed = rms_scale(latent, latent_gain).astype(jnp.bfloat16)
    rotated_key = rope_turn(key_rope.astype(jnp.float32), cosine, sine_table).astype(jnp.bfloat16)
    turned = rope_turn(query_rope.astype(jnp.float32).reshape(SEQ, PAIRS, 2, DR), cosine[:, None, None, :], sine_table[:, None, None, :]).astype(jnp.bfloat16)
    key_rows = jnp.dot(compressed, key_weight.reshape(LATENT, -1), preferred_element_type=jnp.float32).astype(jnp.bfloat16).reshape(SEQ, PAIRS, DK_A + DK_B)
    value_rows = jnp.dot(compressed, value_weight.reshape(LATENT, -1), preferred_element_type=jnp.float32).astype(jnp.bfloat16).reshape(SEQ, PAIRS, DV_A + DV_B)
    scale_one = (DK_A + DR) ** (-0.5)
    scale_two = (DK_B + DR) ** (-0.5)
    block_size = 256

    def attend_block(block_index):
        block_start = block_index * block_size
        query_block = lax.dynamic_slice_in_dim(queries, block_start, block_size, 0)
        turned_block = lax.dynamic_slice_in_dim(turned, block_start, block_size, 0)
        query_places = (block_start + jnp.arange(block_size, dtype=jnp.int32)).astype(jnp.float32)
        visible = query_places[:, None] >= places[None, :]
        part_one = group_attend(query_block[:, :, :DK_A], turned_block[:, :, 0], key_rows[:, :, :DK_A], rotated_key, value_rows[:, :, :DV_A], visible, scale_one)
        part_two = group_attend(query_block[:, :, DK_A:], turned_block[:, :, 1], key_rows[:, :, DK_A:], rotated_key, value_rows[:, :, DV_A:], visible, scale_two)
        return jnp.concatenate([part_one, part_two], axis=2)
    attention = lax.map(attend_block, jnp.arange(SEQ // block_size, dtype=jnp.int32)).reshape(SEQ, PAIRS * (DV_A + DV_B))
    out_flat = out_weight.reshape(PAIRS * (DV_A + DV_B), D)
    run_width = PAIR_DEV * (DV_A + DV_B)

    def add_run(running, run_index):
        columns = lax.dynamic_slice_in_dim(attention, run_index * run_width, run_width, 1)
        weight_rows = lax.dynamic_slice_in_dim(out_flat, run_index * run_width, run_width, 0)
        partial_sum = jnp.dot(columns, weight_rows, preferred_element_type=jnp.float32)
        return (running + lax.optimization_barrier(partial_sum.astype(jnp.bfloat16)).astype(jnp.float32), None)
    head_total, unused = lax.scan(add_run, jnp.zeros((SEQ, D), jnp.float32), jnp.arange(N_TP, dtype=jnp.int32))
    mixed_rows = residual.astype(jnp.float32) + head_total
    normed = rms_scale(mixed_rows, norm_gain).astype(jnp.bfloat16)
    blocks = SEQ // ROWS
    flat_routes = routes.reshape(blocks, ROWS * TOPK)
    onehot = (flat_routes[:, :, None] == jnp.arange(EXPERTS, dtype=jnp.int32)[None, None, :]).astype(jnp.int32)
    rank_within = lax.optimization_barrier(jnp.sum((jnp.cumsum(onehot, axis=1) - onehot) * onehot, axis=2))
    slot_columns = (jnp.arange(blocks, dtype=jnp.int32)[:, None] * CAP + rank_within).reshape(-1).astype(jnp.int32)
    expert_flat = flat_routes.reshape(-1).astype(jnp.int32)
    token_flat = jnp.repeat(jnp.arange(SEQ, dtype=jnp.int32), TOPK)
    token_of = jnp.full((EXPERTS, blocks * CAP), SEQ, dtype=jnp.int32).at[expert_flat, slot_columns].set(token_flat)
    padded = jnp.concatenate([normed, jnp.zeros((1, D), jnp.bfloat16)], axis=0)
    expert_rows = padded[token_of]

    def expert_apply(inputs):
        rows_in, gate_part, up_part, down_part = inputs
        gate_out = jnp.dot(rows_in, gate_part, preferred_element_type=jnp.float32)
        up_out = jnp.dot(rows_in, up_part, preferred_element_type=jnp.float32)
        hidden = (jax.nn.silu(gate_out) * up_out).astype(jnp.bfloat16)
        hidden_runs = hidden.reshape(hidden.shape[0], N_TP, FF_DEV).astype(jnp.float32)
        down_runs = down_part.reshape(N_TP, FF_DEV, D).astype(jnp.float32)
        partial_sum = jnp.einsum('snf,nfd->snd', hidden_runs, down_runs)
        rounded = lax.optimization_barrier(partial_sum.astype(jnp.bfloat16)).astype(jnp.float32)
        return lax.optimization_barrier(jnp.sum(rounded, axis=1)).astype(jnp.bfloat16)
    outputs = lax.map(expert_apply, (expert_rows, gate_weight, up_weight, down_weight))
    picked = outputs[expert_flat, slot_columns].astype(jnp.float32).reshape(SEQ, TOPK, D)
    share_values = expert_share.astype(jnp.float32)
    route_weight = group_gate.astype(jnp.float32)[:, None] * share_values / lax.optimization_barrier(jnp.sum(share_values, axis=1, keepdims=True))
    expert_mix = lax.optimization_barrier(jnp.sum(route_weight[:, :, None] * picked, axis=1))
    return (mixed_rows + expert_mix).astype(jnp.bfloat16)
```

```python
import functools

import jax
import jax.numpy as jnp
from jax import lax
from jax.experimental import pallas as pl
from jax.experimental.pallas import tpu as pltpu
from jax.sharding import PartitionSpec as P

DK_A = 64
DV_A = 64
GROUPS = 4

rope_base = 10000.0
epsilon = 1e-06
floor_score = -1e30
MESH = pl.DeviceIdType.MESH
VM = pl.BlockSpec(memory_space=pltpu.VMEM)


def angle_tables(places, rope_width, repeats):
    steps = jnp.arange(repeats * rope_width // 2, dtype=jnp.int32) % (rope_width // 2)
    frequencies = rope_base ** (-(2 * steps).astype(jnp.float32) / rope_width)
    angles = places[:, None] * frequencies[None, :]
    return (jnp.cos(angles), jnp.sin(angles))


def rms_scale(values, gain_vector):
    values = values.astype(jnp.float32)
    inverse = lax.rsqrt(jnp.mean(values * values, axis=-1, keepdims=True) + epsilon)
    return values * inverse * gain_vector


def greet(targets):
    barrier = pltpu.get_barrier_semaphore()
    for target in targets:
        pl.semaphore_signal(barrier, inc=1, device_id=target, device_id_type=MESH)
    pl.semaphore_wait(barrier, len(targets))


def remote(src, dst, send, recv, target):
    return pltpu.make_async_remote_copy(
        src_ref=src,
        dst_ref=dst,
        send_sem=send,
        recv_sem=recv,
        device_id=target,
        device_id_type=MESH,
    )


def comm_call(kernel, out_shape, scratch, identity, args):
    return pl.pallas_call(
        kernel,
        out_shape=out_shape,
        in_specs=[VM] * len(args),
        out_specs=VM,
        scratch_shapes=scratch,
        compiler_params=pltpu.CompilerParams(
            collective_id=identity, has_side_effects=True, vmem_limit_bytes=48 * 1024 * 1024
        ),
    )(*args)


def greet_some(targets):
    barrier = pltpu.get_barrier_semaphore()
    count = 0
    for here, target in targets:

        @pl.when(here)
        def _():
            pl.semaphore_signal(barrier, inc=1, device_id=target, device_id_type=MESH)

        count = count + jnp.where(here, 1, 0)
    pl.semaphore_wait(barrier, count)


def line(tp_count):
    sp = lax.axis_index("sp")
    tp = lax.axis_index("tp")
    core = lax.rem(tp, 2)
    z = lax.div(tp, 2)
    depth = tp_count // 2
    partner = (sp, tp + 1 - 2 * core)
    return sp, core, z, depth, partner, (sp, tp + 2), (sp, tp - 2), z < depth - 1, z > 0


def moe_kernel(
    sp_count,
    tp_count,
    x_ref,
    pick_ref,
    back_pick_ref,
    gate_ref,
    up_ref,
    down_ref,
    out_ref,
    held,
    picked,
    rows,
    gate,
    up,
    down,
    result,
    swapped,
    summed,
    back,
    mixed,
    stage,
    up_in,
    down_in,
    usend,
    dsend,
    recv,
    ssend,
    srecv,
    fsend,
    frecv,
    wsend,
    wrecv,
    rsend,
    rrecv,
    zsend,
    urecv,
    drecv,
    wsem,
):
    me, core, z, depth, partner, above, below, has_above, has_below = line(tp_count)
    tp = lax.axis_index("tp")
    experts = gate_ref.shape[0]
    model = gate_ref.shape[1]
    tokens = x_ref.shape[0]
    wide = x_ref.shape[1]
    slots = rows.shape[3]
    low = x_ref.dtype
    gather_parts = (slice(0, wide // 256 * 128), slice(wide // 256 * 128, wide))
    parts = (slice(0, model // 256 * 128), slice(model // 256 * 128, model))
    others = [lax.rem(me + k, sp_count) for k in reversed(range(1, sp_count))]
    loads = [
        pltpu.make_async_copy(source, target, wsem.at[i])
        for i, (source, target) in enumerate(((gate_ref, gate), (up_ref, up), (down_ref, down)))
    ]
    greet_some(
        [(True, partner), (has_above, above), (has_below, below)]
        + [(True, (other, tp)) for other in others]
    )

    def move(place, sems, part, target, source=None):
        source = held.at[place] if source is None else source
        return remote(
            source.at[:, gather_parts[part]],
            held.at[place, :, gather_parts[part]],
            sems.at[place, part],
            recv.at[place, part],
            target,
        )

    for part in range(2):

        @pl.when(has_above)
        def _():
            move(z, usend, part, above, x_ref).start()

        @pl.when(has_below)
        def _():
            move(z, dsend, part, below, x_ref).start()

    for load in loads:
        load.start()
    held[z] = x_ref[...]

    def spread(place, other):
        return remote(
            picked.at[place, other],
            rows.at[place, core, me],
            ssend.at[place, other],
            srecv.at[place, me],
            (other, tp),
        )

    def spread_from(place, other):
        return remote(
            picked.at[place, other],
            rows.at[place, core, other],
            ssend.at[place, other],
            srecv.at[place, other],
            (other, tp),
        )

    def share(place, source):
        return remote(
            rows.at[place, core, source],
            rows.at[place, core, source],
            fsend.at[place, source],
            frecv.at[place, source],
            partner,
        )

    def share_own(place):
        return remote(
            picked.at[place, me],
            rows.at[place, core, me],
            fsend.at[place, me],
            frecv.at[place, me],
            partner,
        )

    def shared(place, source):
        return remote(
            rows.at[place, 1 - core, source],
            rows.at[place, 1 - core, source],
            fsend.at[place, source],
            frecv.at[place, source],
            partner,
        )

    def swap(place):
        return remote(
            result.at[place, 1 - core], swapped.at[place], wsend.at[place], wrecv.at[place], partner
        )

    def give(place, other):
        return remote(
            summed.at[place, other],
            back.at[place, me],
            rsend.at[place, other],
            rrecv.at[place, me],
            (other, tp),
        )

    def given(place, other):
        return remote(
            summed.at[place, other],
            back.at[place, other],
            rsend.at[place, other],
            rrecv.at[place, other],
            (other, tp),
        )

    def pass_on(place, part, arrivals, sems, target):
        return remote(
            stage.at[place, :, parts[part]],
            arrivals.at[place, :, parts[part]],
            zsend.at[place, part],
            sems.at[place, part],
            target,
        )

    def rise(place, part):
        return pass_on(place, part, up_in, urecv, above)

    def fall(place, part):
        return pass_on(place, part, down_in, drecv, below)

    def take(k):
        lower, upper = z - k, z + k
        for part in range(2):

            @pl.when((k > 0) & (lower >= 0))
            def _():
                move(lower, usend, part, below).wait_recv()

                @pl.when(has_above)
                def _():
                    move(lower, usend, part, above).start()

            @pl.when((k > 0) & (upper < depth))
            def _():
                move(upper, dsend, part, above).wait_recv()

                @pl.when(has_below)
                def _():
                    move(upper, dsend, part, below).start()

    def choose(place):
        chosen = jnp.dot(pick_ref[place], held[place], preferred_element_type=jnp.float32)
        picked[place] = chosen.astype(low).reshape(sp_count, slots, wide)
        for other in others:
            spread(place, other).start()
        share_own(place).start()
        rows[place, core, me] = picked[place, me]

    def relay(place):
        for other in others:
            spread_from(place, other).wait_recv()
            share(place, other).start()

    def compute(place):
        for source in range(sp_count):
            shared(place, source).wait_recv()
        x = rows[place].reshape(2 * sp_count * slots, wide)
        inputs = x[:, :model]
        tail = x[:, model:].astype(jnp.float32)
        lane = lax.broadcasted_iota(jnp.int32, tail.shape, 1)
        total = None
        for e in range(experts):
            index = me * experts + e
            here = (lane == index) | (lane == index + experts * sp_count)
            scale = jnp.sum(jnp.where(here, tail, 0.0), axis=1, keepdims=True)
            gate_out = jnp.dot(inputs, gate[e], preferred_element_type=jnp.float32)
            up_out = jnp.dot(inputs, up[e], preferred_element_type=jnp.float32)
            hidden = (jax.nn.silu(gate_out) * up_out * scale).astype(low)
            part = jnp.dot(hidden, down[e], preferred_element_type=jnp.float32)
            total = part if e == 0 else total + part
        result[place] = total.astype(low).reshape(2, sp_count, slots, model)
        swap(place).start()

    def settle(place):
        swap(place).wait_recv()
        both = result[place, core].astype(jnp.float32) + swapped[place].astype(jnp.float32)
        summed[place] = both.astype(low)
        for other in others:
            give(place, other).start()
        back[place, me] = summed[place, me]

    def combine(place):
        for other in others:
            given(place, other).wait_recv()
        mixed[place] = jnp.dot(
            back_pick_ref[place],
            back[place].reshape(sp_count * slots, model),
            preferred_element_type=jnp.float32,
        )
        for part in range(2):
            span = parts[part]

            @pl.when((place > z) & (z == 0))
            def _():
                stage[place, :, span] = mixed[place, :, span].astype(low)
                rise(place, part).start()

            @pl.when((place < z) & (z == depth - 1))
            def _():
                stage[place, :, span] = mixed[place, :, span].astype(low)
                fall(place, part).start()

    def at(k, action):
        def one(side, unused):
            place = z + (1 - 2 * side) * k

            @pl.when((place >= 0) & (place < depth) & ((k > 0) | (side == 0)) & (k >= 0))
            def _():
                action(place)

            return unused

        lax.fori_loop(0, 2, one, 0)

    def step(t, unused):
        @pl.when(t < depth)
        def _():
            take(t)
            at(t, choose)

        @pl.when(t == 1)
        def _():
            for load in loads:
                load.wait()

        at(t - 1, relay)
        at(t - 2, settle)
        at(t - 3, combine)
        at(t - 1, compute)
        return unused

    lax.fori_loop(0, depth + 3, step, 0)

    def hop(key, unused):
        high = key - z
        deep = 2 * depth - 2 - key - z
        for part in range(2):
            span = parts[part]

            @pl.when((high > z) & (high < depth) & has_below)
            def _():
                rise(high, part).wait_recv()
                stage[high, :, span] = (
                    mixed[high, :, span] + up_in[high, :, span].astype(jnp.float32)
                ).astype(low)
                rise(high, part).start()

            @pl.when((deep >= 0) & (deep < z) & has_above)
            def _():
                fall(deep, part).wait_recv()
                stage[deep, :, span] = (
                    mixed[deep, :, span] + down_in[deep, :, span].astype(jnp.float32)
                ).astype(low)
                fall(deep, part).start()

        return unused

    lax.fori_loop(1, 2 * depth - 2, hop, 0)
    for part in range(2):
        span = parts[part]
        out_ref[:, span] = mixed[z, :, span]

        @pl.when(has_below)
        def _():
            rise(z, part).wait_recv()
            out_ref[:, span] += up_in[z, :, span].astype(jnp.float32)

        @pl.when(has_above)
        def _():
            fall(z, part).wait_recv()
            out_ref[:, span] += down_in[z, :, span].astype(jnp.float32)

    def finish(place, unused):
        for part in range(2):

            @pl.when(has_above & (place <= z))
            def _():
                move(place, usend, part, above).wait_send()

            @pl.when(has_below & (place >= z))
            def _():
                move(place, dsend, part, below).wait_send()

            @pl.when(place > z)
            def _():
                rise(place, part).wait_send()

            @pl.when(place < z)
            def _():
                fall(place, part).wait_send()

        for other in others:
            spread(place, other).wait_send()
            share(place, other).wait_send()
            give(place, other).wait_send()
        share_own(place).wait_send()
        swap(place).wait_send()
        return unused

    lax.fori_loop(0, depth, finish, 0)


def moe(x, pick, back_pick, gate_weight, up_weight, down_weight, sp_count, tp_count, identity):
    dma = pltpu.SemaphoreType.DMA
    depth = tp_count // 2
    model = gate_weight.shape[1]
    tokens, wide = x.shape
    slots = pick.shape[1] // sp_count
    low = x.dtype
    anywhere = pl.BlockSpec(memory_space=pl.ANY)
    each = dma((depth, sp_count))
    two = dma((depth, 2))
    block = pltpu.VMEM((depth, tokens, model), low)
    group = pltpu.VMEM((depth, sp_count, slots, model), low)
    return pl.pallas_call(
        functools.partial(moe_kernel, sp_count, tp_count),
        out_shape=jax.ShapeDtypeStruct((tokens, model), jnp.float32),
        in_specs=[VM, VM, VM, anywhere, anywhere, anywhere],
        out_specs=VM,
        scratch_shapes=[
            pltpu.VMEM((depth, tokens, wide), low),
            pltpu.VMEM((depth, sp_count, slots, wide), low),
            pltpu.VMEM((depth, 2, sp_count, slots, wide), low),
            pltpu.VMEM(gate_weight.shape, gate_weight.dtype),
            pltpu.VMEM(up_weight.shape, up_weight.dtype),
            pltpu.VMEM(down_weight.shape, down_weight.dtype),
            pltpu.VMEM((depth, 2, sp_count, slots, model), low),
            group,
            group,
            group,
            pltpu.VMEM((depth, tokens, model), jnp.float32),
            block,
            block,
            block,
            two,
            two,
            two,
            each,
            each,
            each,
            each,
            dma((depth,)),
            dma((depth,)),
            each,
            each,
            two,
            two,
            two,
            dma((3,)),
        ],
        compiler_params=pltpu.CompilerParams(
            collective_id=identity, has_side_effects=True, vmem_limit_bytes=60 * 1024 * 1024
        ),
    )(x, pick, back_pick, gate_weight, up_weight, down_weight)


def reduce_tp_kernel(
    tp_count, x_ref, out_ref, partner_in, stage, up_in, down_in, send, recv, zsend, urecv, drecv
):
    sp, core, z, depth, partner, above, below, has_above, has_below = line(tp_count)
    greet_some([(True, partner), (has_above, above), (has_below, below)])

    middle = x_ref.shape[2] // 256 * 128
    parts = (slice(0, middle), slice(middle, x_ref.shape[2]))

    def swap(place, part):
        return remote(
            x_ref.at[place * 2 + 1 - core, :, parts[part]],
            partner_in.at[place, :, parts[part]],
            send.at[place, part],
            recv.at[place, part],
            partner,
        )

    def pass_on(place, part, arrivals, sems, target):
        return remote(
            stage.at[place, :, parts[part]],
            arrivals.at[place, :, parts[part]],
            zsend.at[place, part],
            sems.at[place, part],
            target,
        )

    def up(place, part):
        return pass_on(place, part, up_in, urecv, above)

    def down(place, part):
        return pass_on(place, part, down_in, drecv, below)

    def pair_sum(place, part):
        swap(place, part).wait_recv()
        mine = x_ref[place * 2 + core, :, parts[part]].astype(jnp.float32)
        return mine + partner_in[place, :, parts[part]].astype(jnp.float32)

    for j in range(depth):
        for part in range(2):
            swap(depth - 1 - j, part).start()
            if depth - 1 - j > j:
                swap(j, part).start()
        if depth - 1 - j <= j + 1:
            break

    for j in range(depth - 1):
        high, low = depth - 1 + z - j, j + z + 1 - depth
        for part in range(2):
            span = parts[part]

            @pl.when(z <= j)
            def _():
                stage[high, :, span] = pair_sum(high, part).astype(stage.dtype)

                @pl.when(has_below)
                def _():
                    up(high, part).wait_recv()
                    stage[high, :, span] = (
                        stage[high, :, span].astype(jnp.float32)
                        + up_in[high, :, span].astype(jnp.float32)
                    ).astype(stage.dtype)

                up(high, part).start()

            @pl.when(low >= 0)
            def _():
                stage[low, :, span] = pair_sum(low, part).astype(stage.dtype)

                @pl.when(has_above)
                def _():
                    down(low, part).wait_recv()
                    stage[low, :, span] = (
                        stage[low, :, span].astype(jnp.float32)
                        + down_in[low, :, span].astype(jnp.float32)
                    ).astype(stage.dtype)

                down(low, part).start()

    for part in range(2):
        span = parts[part]
        out_ref[:, span] = pair_sum(z, part)

        @pl.when(has_below)
        def _():
            up(z, part).wait_recv()
            out_ref[:, span] += up_in[z, :, span].astype(jnp.float32)

        @pl.when(has_above)
        def _():
            down(z, part).wait_recv()
            out_ref[:, span] += down_in[z, :, span].astype(jnp.float32)

    for place in range(depth):
        for part in range(2):
            swap(place, part).wait_send()

            @pl.when(place > z)
            def _():
                up(place, part).wait_send()

            @pl.when(place < z)
            def _():
                down(place, part).wait_send()


def reduce_tp(x, tp_count, identity):
    block = x.shape[1:]
    depth = tp_count // 2
    buffer = pltpu.VMEM((depth,) + block, x.dtype)
    return comm_call(
        functools.partial(reduce_tp_kernel, tp_count),
        jax.ShapeDtypeStruct(block, jnp.float32),
        [buffer] * 4 + [pltpu.SemaphoreType.DMA((depth, 2))] * 5,
        identity,
        (x,),
    )


NT = (((1,), (1,)), ((), ()))


def attend_kernel(
    rope_width,
    sp_count,
    x_ref,
    q_ref,
    qr_ref,
    cos_ref,
    sin_ref,
    turn_ref,
    wk_ref,
    wv_ref,
    wo_ref,
    out_ref,
    turned,
    keys,
    values,
    tops,
    sums,
    acc,
    held,
    send,
    recv,
    fsend,
):
    me = lax.axis_index("sp")
    tp = lax.axis_index("tp")
    core = lax.rem(tp, 2)
    partner = (me, tp + 1 - 2 * core)
    tokens, width = q_ref.shape
    half = tokens // 2
    greet([(lax.rem(me + k, sp_count), tp) for k in range(1, sp_count)] + [partner])
    mine = pl.ds(pl.multiple_of(core * half, half), half)
    other = pl.ds(pl.multiple_of((1 - core) * half, half), half)

    def outgoing(to):
        return remote(
            x_ref.at[mine], held.at[me, mine], send.at[to], recv.at[me, core], (to, tp)
        )

    def incoming(source):
        return remote(
            x_ref.at[mine], held.at[source, mine], send.at[source], recv.at[source, core], partner
        )

    def forward(source):
        return remote(
            held.at[source, mine],
            held.at[source, mine],
            fsend.at[source],
            recv.at[source, core],
            partner,
        )

    def forwarded(source):
        return remote(
            held.at[source, other],
            held.at[source, other],
            fsend.at[source],
            recv.at[source, 1 - core],
            partner,
        )

    for to in reversed(range(sp_count)):

        @pl.when(to > me)
        def _():
            outgoing(to).start()

    latent = wk_ref.shape[0]
    pair_width = width // (qr_ref.shape[1] // (2 * rope_width))
    pairs = width // pair_width
    raw = qr_ref[...]
    swapped = jnp.dot(raw, turn_ref[...], preferred_element_type=jnp.float32)
    turned[...] = (raw.astype(jnp.float32) * cos_ref[...] + swapped * sin_ref[...]).astype(
        turned.dtype
    )
    scales = ((DK_A + rope_width) ** (-0.5), (pair_width - DK_A + rope_width) ** (-0.5))

    def block(index, first):
        compressed = x_ref[:, :latent] if first else held[index, :, :latent]
        rope = x_ref[:, latent:] if first else held[index, :, latent:]
        keys[...] = jnp.dot(compressed, wk_ref[...], preferred_element_type=jnp.float32).astype(
            keys.dtype
        )
        values[...] = jnp.dot(compressed, wv_ref[...], preferred_element_type=jnp.float32).astype(
            values.dtype
        )
        for pair in range(pairs):
            span = slice(pair * pair_width, (pair + 1) * pair_width)
            lane = lax.broadcasted_iota(jnp.int32, (tokens, pair_width), 1)
            rope_lane = lax.broadcasted_iota(jnp.int32, turned.shape, 1)
            factors, updates = [], []
            for group in range(2):
                head = pair * 2 + group
                chosen = (lane < DK_A) if group == 0 else (lane >= DK_A)
                query = jnp.where(chosen, q_ref[:, span], jnp.zeros((), q_ref.dtype))
                low = head * rope_width
                query_rope = jnp.where(
                    (rope_lane >= low) & (rope_lane < low + rope_width),
                    turned[...],
                    jnp.zeros((), turned.dtype),
                )
                scores = lax.dot_general(
                    query, keys[:, span], NT, preferred_element_type=jnp.float32
                ) + lax.dot_general(query_rope, rope, NT, preferred_element_type=jnp.float32)
                scores = scores * scales[group]
                if first:
                    row = lax.broadcasted_iota(jnp.int32, (tokens, tokens), 0)
                    column = lax.broadcasted_iota(jnp.int32, (tokens, tokens), 1)
                    scores = jnp.where(row >= column, scores, floor_score)
                    top = jnp.max(scores, axis=1, keepdims=True)
                else:
                    old = tops[head]
                    top = jnp.maximum(old, jnp.max(scores, axis=1, keepdims=True))
                    factors.append(jnp.exp(old - top))
                weights = jnp.exp(scores - top)
                total = jnp.sum(weights, axis=1, keepdims=True)
                tops[head] = top
                sums[head] = total if first else sums[head] * factors[-1] + total
                updates.append(
                    jnp.dot(
                        weights.astype(values.dtype),
                        values[:, span],
                        preferred_element_type=jnp.float32,
                    )
                )
            value_lane = lane < DV_A
            update = jnp.where(value_lane, updates[0], updates[1])
            if first:
                acc[:, span] = update
            else:
                acc[:, span] = (
                    acc[:, span] * jnp.where(value_lane, factors[0], factors[1]) + update
                )

    block(me, True)

    def step(i, unused):
        index = me - 1 - i
        incoming(index).wait_recv()
        forward(index).start()
        forwarded(index).wait_recv()
        block(index, False)
        return unused

    lax.fori_loop(0, me, step, 0)
    for pair in range(pairs):
        span = slice(pair * pair_width, (pair + 1) * pair_width)
        lane = lax.broadcasted_iota(jnp.int32, (tokens, pair_width), 1)
        bottom = jnp.where(lane < DV_A, sums[pair * 2], sums[pair * 2 + 1])
        keys[:, span] = (acc[:, span] / bottom).astype(keys.dtype)
    piece = 512
    for start in range(0, wo_ref.shape[1], piece):
        out_ref[:, start : start + piece] = jnp.dot(
            keys[...], wo_ref[:, start : start + piece], preferred_element_type=jnp.float32
        ).astype(out_ref.dtype)
    for place in range(sp_count):

        @pl.when(place < me)
        def _():
            forward(place).wait_send()

        @pl.when(place > me)
        def _():
            outgoing(place).wait_send()


def local(
    residual,
    queries,
    query_rope,
    latent,
    key_rope,
    latent_gain,
    key_weight,
    value_weight,
    out_weight,
    norm_gain,
    routes,
    group_gate,
    expert_share,
    gate_weight,
    up_weight,
    down_weight,
):
    tokens = queries.shape[0]
    pair_dev = queries.shape[1]
    sp_count = lax.axis_size("sp")
    tp_count = lax.axis_size("tp")
    row_count = tokens // tp_count
    rope_width = key_rope.shape[1]
    half = rope_width // 2
    copies = pair_dev * 2
    latent_width = latent.shape[1]
    model = residual.shape[1]
    low = jnp.bfloat16

    first_place = lax.axis_index("sp") * tokens
    places = (first_place + jnp.arange(tokens, dtype=jnp.int32)).astype(jnp.float32)
    cosine, sine = angle_tables(places, rope_width, 2 * copies)
    index = jnp.arange(copies * rope_width, dtype=jnp.int32)
    source = jnp.where(index % rope_width < half, index + half, index - half)
    sign = jnp.where(index % rope_width < half, -1.0, 1.0)
    turn = jnp.where(index[:, None] == source[None, :], sign[None, :], 0.0).astype(low)
    key_raw = jnp.tile(key_rope, (1, copies))
    rotated = (
        key_raw.astype(jnp.float32) * cosine
        + jnp.dot(key_raw, turn, preferred_element_type=jnp.float32) * sine
    ).astype(low)
    compressed = rms_scale(latent, latent_gain).astype(low)
    own_latent = jnp.concatenate([compressed, rotated], axis=1)

    width = pair_dev * queries.shape[2]
    scratch = [
        pltpu.VMEM((tokens, copies * rope_width), low),
        pltpu.VMEM((tokens, width), low),
        pltpu.VMEM((tokens, width), low),
        pltpu.VMEM((copies, tokens, 1), jnp.float32),
        pltpu.VMEM((copies, tokens, 1), jnp.float32),
        pltpu.VMEM((tokens, width), jnp.float32),
        pltpu.VMEM((sp_count,) + own_latent.shape, low),
        pltpu.SemaphoreType.DMA((sp_count,)),
        pltpu.SemaphoreType.DMA((sp_count, 2)),
        pltpu.SemaphoreType.DMA((sp_count,)),
    ]
    partial = pl.pallas_call(
        functools.partial(attend_kernel, rope_width, sp_count),
        out_shape=jax.ShapeDtypeStruct((tokens, model), low),
        in_specs=[VM] * 9,
        out_specs=VM,
        scratch_shapes=scratch,
        compiler_params=pltpu.CompilerParams(
            collective_id=0, has_side_effects=True, vmem_limit_bytes=48 * 1024 * 1024
        ),
    )(
        own_latent,
        queries.reshape(tokens, width),
        query_rope.reshape(tokens, copies * rope_width),
        cosine,
        sine,
        turn,
        key_weight.reshape(latent_width, -1),
        value_weight.reshape(latent_width, -1),
        out_weight.reshape(width, model),
    )
    head_total = reduce_tp(partial.reshape(tp_count, row_count, model), tp_count, 1)
    mixed_rows = residual.astype(jnp.float32) + head_total
    normed = rms_scale(mixed_rows, norm_gain).astype(low)

    experts_dev = gate_weight.shape[0]
    experts_all = experts_dev * sp_count
    top_count = routes.shape[1]
    depth = tp_count // 2
    capacity = max(2, 3 * row_count * top_count // (2 * experts_all))
    slots = experts_dev * capacity
    if experts_all // GROUPS == experts_dev == top_count:
        slots = capacity
    slots = -(-slots // 8) * 8
    tp = lax.axis_index("tp")
    own = lax.dynamic_slice_in_dim(routes, tp * row_count, row_count, 0)
    route_weight = group_gate[:, None] * expert_share / jnp.sum(expert_share, axis=1, keepdims=True)
    expert_ids = jnp.arange(experts_all, dtype=jnp.int32)
    named = own[:, :, None] == expert_ids[None, None, :]
    table = jnp.sum(jnp.where(named, route_weight[:, :, None], 0.0), axis=1)
    weight_high = table.astype(low)
    weight_low = (table - weight_high.astype(jnp.float32)).astype(low)
    extra = jnp.concatenate([weight_high, weight_low], axis=1)
    extra = jnp.pad(extra, ((0, 0), (0, 128 - extra.shape[1])))

    column = lax.dynamic_index_in_dim(
        routes.reshape(depth, 2, row_count, top_count), lax.rem(tp, 2), 1, keepdims=False
    )
    goal = column // experts_dev
    member = jnp.any(goal[:, :, :, None] == jnp.arange(sp_count, dtype=jnp.int32), axis=2)
    row = jnp.arange(row_count, dtype=jnp.int32)
    earlier = (row[:, None] > row[None, :]).astype(low)
    rank = jnp.einsum(
        "rq,zqs->zrs", earlier, member.astype(low), preferred_element_type=jnp.float32
    )
    rank = jnp.where(member, rank.astype(jnp.int32), -1)
    slot_ids = jnp.arange(slots, dtype=jnp.int32)
    back_pick = (rank[:, :, :, None] == slot_ids).astype(low)
    back_pick = back_pick.reshape(depth, row_count, sp_count * slots)
    pick = (jnp.swapaxes(rank, 1, 2)[:, :, None, :] == slot_ids[:, None]).astype(low)
    pick = pick.reshape(depth, sp_count * slots, row_count)
    x = jnp.concatenate([normed, extra], axis=1)
    expert_mix = moe(
        x, pick, back_pick, gate_weight, up_weight, down_weight, sp_count, tp_count, 3
    )
    return (mixed_rows + expert_mix).astype(low)


def solution(mesh):
    return jax.shard_map(
        local,
        mesh=mesh,
        in_specs=(
            P(("sp", "tp"), None),
            P("sp", "tp", None),
            P("sp", "tp", None),
            P("sp", None),
            P("sp", None),
            P(),
            P(None, "tp", None),
            P(None, "tp", None),
            P("tp", None, None),
            P(),
            P("sp", None),
            P(("sp", "tp")),
            P(("sp", "tp"), None),
            P("sp", None, "tp"),
            P("sp", None, "tp"),
            P("sp", "tp", None),
        ),
        out_specs=P(("sp", "tp"), None),
        check_vma=False,
    )
```

```python
import functools

import jax
import jax.numpy as jnp
from jax import lax
from jax.experimental import pallas as pl
from jax.experimental.pallas import tpu as pltpu
from jax.sharding import PartitionSpec as P

DK_A = 64
DV_A = 64
GROUPS = 4

rope_base = 10000.0
epsilon = 1e-06
floor_score = -1e30
MESH = pl.DeviceIdType.MESH
VM = pl.BlockSpec(memory_space=pltpu.VMEM)


def angle_tables(places, rope_width):
    steps = jnp.arange(rope_width // 2, dtype=jnp.int32)
    frequencies = rope_base ** (-(2 * steps).astype(jnp.float32) / rope_width)
    angles = places[None, :] * frequencies[:, None]
    return (jnp.cos(angles), jnp.sin(angles))


def rms_scale(values, gain_vector):
    values = values.astype(jnp.float32)
    inverse = lax.rsqrt(jnp.mean(values * values, axis=-1, keepdims=True) + epsilon)
    return values * inverse * gain_vector


def remote(src, dst, send, recv, target):
    return pltpu.make_async_remote_copy(
        src_ref=src,
        dst_ref=dst,
        send_sem=send,
        recv_sem=recv,
        device_id=target,
        device_id_type=MESH,
    )


def greet_some(targets):
    barrier = pltpu.get_barrier_semaphore()
    count = 0
    for here, target in targets:

        @pl.when(here)
        def _():
            pl.semaphore_signal(barrier, inc=1, device_id=target, device_id_type=MESH)

        count = count + jnp.where(here, 1, 0)
    pl.semaphore_wait(barrier, count)


def line(tp_count):
    sp = lax.axis_index("sp")
    tp = lax.axis_index("tp")
    core = lax.rem(tp, 2)
    z = lax.div(tp, 2)
    depth = tp_count // 2
    partner = (sp, tp + 1 - 2 * core)
    return sp, core, z, depth, partner, (sp, tp + 2), (sp, tp - 2), z < depth - 1, z > 0


def moe_kernel(
    sp_count,
    tp_count,
    heads_ref,
    residual_ref,
    norm_gain_ref,
    extra_ref,
    rank_ref,
    gate_ref,
    up_ref,
    down_ref,
    out_ref,
    own,
    token_rows,
    pick,
    back_pick,
    held,
    picked,
    rows,
    gate,
    up,
    down,
    result,
    swapped,
    summed,
    back,
    mixed,
    stage,
    up_in,
    down_in,
    usend,
    dsend,
    recv,
    ssend,
    srecv,
    fsend,
    frecv,
    wsend,
    wrecv,
    rsend,
    rrecv,
    zsend,
    urecv,
    drecv,
    wsem,
):
    me, core, z, depth, partner, above, below, has_above, has_below = line(tp_count)
    tp = lax.axis_index("tp")
    experts = gate_ref.shape[0]
    model = gate_ref.shape[1]
    tokens, wide = own.shape
    slots = rows.shape[3]
    low = own.dtype
    gather_parts = (slice(0, wide // 256 * 128), slice(wide // 256 * 128, wide))
    parts = (slice(0, model // 256 * 128), slice(model // 256 * 128, model))
    others = [lax.rem(me + k, sp_count) for k in reversed(range(1, sp_count))]
    loads = [
        pltpu.make_async_copy(source, target, wsem.at[i])
        for i, (source, target) in enumerate(((gate_ref, gate), (up_ref, up), (down_ref, down)))
    ]
    for load in loads:
        load.start()
    total = residual_ref[...].astype(jnp.float32) + heads_ref[...]
    token_rows[...] = total
    own[:, :model] = rms_scale(total, norm_gain_ref[...]).astype(low)
    own[:, model:] = extra_ref[...]
    greet_some(
        [(True, partner), (has_above, above), (has_below, below)]
        + [(True, (other, tp)) for other in others]
    )

    def move(place, sems, part, target, source=None):
        source = held.at[place] if source is None else source
        return remote(
            source.at[:, gather_parts[part]],
            held.at[place, :, gather_parts[part]],
            sems.at[place, part],
            recv.at[place, part],
            target,
        )

    for part in range(2):

        @pl.when(has_above)
        def _():
            move(z, usend, part, above, own).start()

        @pl.when(has_below)
        def _():
            move(z, dsend, part, below, own).start()

    held[z] = own[...]
    slot = lax.broadcasted_iota(jnp.int32, (slots, tokens), 0)
    for place in range(depth):
        chosen = [
            jnp.where(rank_ref[place, source : source + 1] == slot, 1.0, 0.0)
            for source in range(sp_count)
        ]
        chosen = jnp.concatenate(chosen, axis=0)
        pick[place] = chosen.astype(low)
        back_pick[place] = chosen.T.astype(low)

    def send_to(source, target, sends, recvs, place, part, mark, arrive, device):
        return remote(
            source, target, sends.at[place, mark, part], recvs.at[place, arrive, part], device
        )

    def spread(place, part, other, arrive=None):
        arrive = me if arrive is None else arrive
        span = gather_parts[part]
        return send_to(
            picked.at[place, other, :, span],
            rows.at[place, core, arrive, :, span],
            ssend,
            srecv,
            place,
            part,
            other,
            arrive,
            (other, tp),
        )

    def share(place, part, source, own_rows=False):
        span = gather_parts[part]
        target = rows.at[place, core, source, :, span]
        start = picked.at[place, source, :, span] if own_rows else target
        return send_to(start, target, fsend, frecv, place, part, source, source, partner)

    def shared(place, part, source):
        target = rows.at[place, 1 - core, source, :, gather_parts[part]]
        return send_to(target, target, fsend, frecv, place, part, source, source, partner)

    def swap(place, part):
        return remote(
            result.at[place, 1 - core, :, :, parts[part]],
            swapped.at[place, :, :, parts[part]],
            wsend.at[place, part],
            wrecv.at[place, part],
            partner,
        )

    def give(place, part, other, arrive=None):
        arrive = me if arrive is None else arrive
        span = parts[part]
        return send_to(
            summed.at[place, other, :, span],
            back.at[place, arrive, :, span],
            rsend,
            rrecv,
            place,
            part,
            other,
            arrive,
            (other, tp),
        )

    def pass_on(place, part, arrivals, sems, target):
        return remote(
            stage.at[place, :, parts[part]],
            arrivals.at[place, :, parts[part]],
            zsend.at[place, part],
            sems.at[place, part],
            target,
        )

    def rise(place, part):
        return pass_on(place, part, up_in, urecv, above)

    def fall(place, part):
        return pass_on(place, part, down_in, drecv, below)

    def take(k, part):
        lower, upper = z - k, z + k

        @pl.when((k > 0) & (lower >= 0))
        def _():
            move(lower, usend, part, below).wait_recv()

            @pl.when(has_above)
            def _():
                move(lower, usend, part, above).start()

        @pl.when((k > 0) & (upper < depth))
        def _():
            move(upper, dsend, part, above).wait_recv()

            @pl.when(has_below)
            def _():
                move(upper, dsend, part, below).start()

    def choose(place, part):
        span = gather_parts[part]
        chosen = jnp.dot(pick[place], held[place, :, span], preferred_element_type=jnp.float32)
        picked[place, :, :, span] = chosen.astype(low).reshape(
            sp_count, slots, span.stop - span.start
        )
        for other in others:
            spread(place, part, other).start()
        share(place, part, me, True).start()
        rows[place, core, me, :, span] = picked[place, me, :, span]

    def relay(place, part):
        for other in others:
            spread(place, part, other, other).wait_recv()
            share(place, part, other).start()

    def compute(place):
        for part in range(2):
            for source in range(sp_count):
                shared(place, part, source).wait_recv()
        x = rows[place].reshape(2 * sp_count * slots, wide)
        inputs = x[:, :model]
        tail = x[:, model:].astype(jnp.float32)
        lane = lax.broadcasted_iota(jnp.int32, tail.shape, 1)
        hidden = []
        for e in range(experts):
            index = me * experts + e
            here = (lane == index) | (lane == index + experts * sp_count)
            scale = jnp.sum(jnp.where(here, tail, 0.0), axis=1, keepdims=True)
            gate_out = jnp.dot(inputs, gate[e], preferred_element_type=jnp.float32)
            up_out = jnp.dot(inputs, up[e], preferred_element_type=jnp.float32)
            hidden.append((jax.nn.silu(gate_out) * up_out * scale).astype(low))
        for part in range(2):
            span = parts[part]
            total = jnp.dot(hidden[0], down[0, :, span], preferred_element_type=jnp.float32)
            for e in range(1, experts):
                total += jnp.dot(hidden[e], down[e, :, span], preferred_element_type=jnp.float32)
            result[place, :, :, :, span] = total.astype(low).reshape(
                2, sp_count, slots, span.stop - span.start
            )
            swap(place, part).start()

    def settle(place, part):
        span = parts[part]
        swap(place, part).wait_recv()
        kept = result[place, core, :, :, span].astype(jnp.float32)
        both = kept + swapped[place, :, :, span].astype(jnp.float32)
        summed[place, :, :, span] = both.astype(low)
        for other in others:
            give(place, part, other).start()
        back[place, me, :, span] = summed[place, me, :, span]

    def combine(place, part):
        span = parts[part]
        for other in others:
            give(place, part, other, other).wait_recv()
        mixed[place, :, span] = jnp.dot(
            back_pick[place],
            back[place, :, :, span].reshape(sp_count * slots, span.stop - span.start),
            preferred_element_type=jnp.float32,
        )

        @pl.when((place > z) & (z == 0))
        def _():
            stage[place, :, span] = mixed[place, :, span].astype(low)
            rise(place, part).start()

        @pl.when((place < z) & (z == depth - 1))
        def _():
            stage[place, :, span] = mixed[place, :, span].astype(low)
            fall(place, part).start()

    def at(k, action):
        def one(side, unused):
            place = z + (1 - 2 * side) * k

            @pl.when((place >= 0) & (place < depth) & ((k > 0) | (side == 0)) & (k >= 0))
            def _():
                action(place)

            return unused

        lax.fori_loop(0, 2, one, 0)

    def step(t, unused):
        @pl.when(t < depth)
        def _():
            for part in range(2):
                take(t, part)
                at(t, lambda place: choose(place, part))

        @pl.when(t == 1)
        def _():
            for load in loads:
                load.wait()

        for action, late in ((relay, 1), (settle, 2), (combine, 3)):
            for part in range(2):
                at(t - late, lambda place: action(place, part))
        at(t - 1, compute)
        return unused

    lax.fori_loop(0, depth + 3, step, 0)

    def hop(key, unused):
        high = key - z
        deep = 2 * depth - 2 - key - z
        for part in range(2):
            span = parts[part]

            @pl.when((high > z) & (high < depth) & has_below)
            def _():
                rise(high, part).wait_recv()
                stage[high, :, span] = (
                    mixed[high, :, span] + up_in[high, :, span].astype(jnp.float32)
                ).astype(low)
                rise(high, part).start()

            @pl.when((deep >= 0) & (deep < z) & has_above)
            def _():
                fall(deep, part).wait_recv()
                stage[deep, :, span] = (
                    mixed[deep, :, span] + down_in[deep, :, span].astype(jnp.float32)
                ).astype(low)
                fall(deep, part).start()

        return unused

    lax.fori_loop(1, 2 * depth - 2, hop, 0)
    for part in range(2):
        span = parts[part]
        token_rows[:, span] += mixed[z, :, span]

        @pl.when(has_below)
        def _():
            rise(z, part).wait_recv()
            token_rows[:, span] += up_in[z, :, span].astype(jnp.float32)

        @pl.when(has_above)
        def _():
            fall(z, part).wait_recv()
            token_rows[:, span] += down_in[z, :, span].astype(jnp.float32)

        out_ref[:, span] = token_rows[:, span].astype(low)

    def finish(place, unused):
        for part in range(2):

            @pl.when(has_above & (place <= z))
            def _():
                move(place, usend, part, above).wait_send()

            @pl.when(has_below & (place >= z))
            def _():
                move(place, dsend, part, below).wait_send()

            @pl.when(place > z)
            def _():
                rise(place, part).wait_send()

            @pl.when(place < z)
            def _():
                fall(place, part).wait_send()

            for other in others:
                spread(place, part, other).wait_send()
                share(place, part, other).wait_send()
                give(place, part, other).wait_send()
            share(place, part, me, True).wait_send()
            swap(place, part).wait_send()
        return unused

    lax.fori_loop(0, depth, finish, 0)


def moe(
    heads,
    residual,
    norm_gain,
    extra,
    rank,
    slots,
    gate_weight,
    up_weight,
    down_weight,
    sp_count,
    tp_count,
    identity,
):
    dma = pltpu.SemaphoreType.DMA
    depth = tp_count // 2
    tokens, model = residual.shape
    wide = model + extra.shape[1]
    low = residual.dtype
    anywhere = pl.BlockSpec(memory_space=pl.ANY)
    each = dma((depth, sp_count, 2))
    two = dma((depth, 2))
    block = pltpu.VMEM((depth, tokens, model), low)
    group = pltpu.VMEM((depth, sp_count, slots, model), low)
    return pl.pallas_call(
        functools.partial(moe_kernel, sp_count, tp_count),
        out_shape=jax.ShapeDtypeStruct((tokens, model), low),
        in_specs=[VM, VM, VM, VM, VM, anywhere, anywhere, anywhere],
        out_specs=VM,
        scratch_shapes=[
            pltpu.VMEM((tokens, wide), low),
            pltpu.VMEM((tokens, model), jnp.float32),
            pltpu.VMEM((depth, sp_count * slots, tokens), low),
            pltpu.VMEM((depth, tokens, sp_count * slots), low),
            pltpu.VMEM((depth, tokens, wide), low),
            pltpu.VMEM((depth, sp_count, slots, wide), low),
            pltpu.VMEM((depth, 2, sp_count, slots, wide), low),
            pltpu.VMEM(gate_weight.shape, gate_weight.dtype),
            pltpu.VMEM(up_weight.shape, up_weight.dtype),
            pltpu.VMEM(down_weight.shape, down_weight.dtype),
            pltpu.VMEM((depth, 2, sp_count, slots, model), low),
            group,
            group,
            group,
            pltpu.VMEM((depth, tokens, model), jnp.float32),
            block,
            block,
            block,
            two,
            two,
            two,
            each,
            each,
            each,
            each,
            two,
            two,
            each,
            each,
            two,
            two,
            two,
            dma((3,)),
        ],
        compiler_params=pltpu.CompilerParams(
            collective_id=identity, has_side_effects=True, vmem_limit_bytes=60 * 1024 * 1024
        ),
    )(heads, residual, norm_gain[None, :], extra, rank, gate_weight, up_weight, down_weight)


NT = (((1,), (1,)), ((), ()))


def attend_kernel(
    rope_width,
    sp_count,
    tp_count,
    latent_ref,
    gain_ref,
    key_rope_ref,
    q_ref,
    q_rope_ref,
    cos_ref,
    sin_ref,
    wk_ref,
    wv_ref,
    wo_ref,
    out_ref,
    latent,
    queries,
    wk_raw,
    wv_raw,
    wo,
    own,
    held,
    qx,
    wk,
    wvt,
    kx,
    vt,
    tops,
    sums,
    acc,
    attention,
    partial,
    partner_in,
    stage,
    up_in,
    down_in,
    wsem,
    send,
    recv,
    fsend,
    psend,
    precv,
    zsend,
    urecv,
    drecv,
):
    me, core, z, depth, partner, above, below, has_above, has_below = line(tp_count)
    tp = lax.axis_index("tp")
    tokens, width = latent.shape
    pairs, pair_width = queries.shape[1:]
    half = tokens // 2
    low = own.dtype
    loads = [
        pltpu.make_async_copy(source, target, wsem.at[i])
        for i, (source, target) in enumerate(
            (
                (latent_ref, latent),
                (q_ref, queries),
                (wk_ref, wk_raw),
                (wv_ref, wv_raw),
                (wo_ref, wo),
            )
        )
    ]
    for load in loads:
        load.start()
    mine = pl.ds(pl.multiple_of(core * half, half), half)
    other = pl.ds(pl.multiple_of((1 - core) * half, half), half)

    def outgoing(to):
        return remote(own.at[mine], held.at[me, mine], send.at[to], recv.at[me, core], (to, tp))

    def incoming(source):
        return remote(
            own.at[mine], held.at[source, mine], send.at[source], recv.at[source, core], partner
        )

    def forward(source):
        return remote(
            held.at[source, mine],
            held.at[source, mine],
            fsend.at[source],
            recv.at[source, core],
            partner,
        )

    def forwarded(source):
        return remote(
            held.at[source, other],
            held.at[source, other],
            fsend.at[source],
            recv.at[source, 1 - core],
            partner,
        )

    turn = rope_width // 2
    cosine, sine = cos_ref[...], sin_ref[...]

    def rotate(upper, lower):
        return upper * cosine - lower * sine, lower * cosine + upper * sine

    raw = key_rope_ref[...].astype(jnp.float32)
    rotated = list(rotate(raw[:turn], raw[turn:]))
    own[:, width:] = jnp.concatenate(rotated * (128 // rope_width), axis=0).T.astype(low)
    loads[0].wait()
    values = latent[...].astype(jnp.float32)
    inverse = lax.rsqrt(jnp.mean(values * values, axis=-1, keepdims=True) + epsilon)
    own[:, :width] = (values * inverse * gain_ref[...]).astype(low)

    greet_some(
        [(True, partner), (has_above, above), (has_below, below)]
        + [(True, (lax.rem(me + k, sp_count), tp)) for k in range(1, sp_count)]
    )
    for to in reversed(range(sp_count)):

        @pl.when(to > me)
        def _():
            outgoing(to).start()

    def merge(one, two):
        lane = lax.broadcasted_iota(jnp.int32, one.shape, 1)
        return jnp.where(lane < DK_A, one, two)

    for load in loads[1:]:
        load.wait()
    gap = jnp.zeros((DK_A - rope_width, tokens), jnp.float32)
    for pair in range(pairs):
        rope = q_rope_ref[pair].astype(jnp.float32)
        first = list(rotate(rope[:turn], rope[turn:rope_width]))
        second = list(rotate(rope[rope_width : rope_width + turn], rope[rope_width + turn :]))
        turned = jnp.concatenate(second + [gap] + first + [gap], axis=0).T.astype(low)
        qx[pair, :, 128:] = queries[:, pair, :]
        query = qx[pair, :, 128:256]
        qx[pair, :, :128] = merge(query, turned)
        qx[pair, :, 128:256] = merge(turned, query)
        wk[pair] = wk_raw[:, pair, :]
        wvt[pair] = wv_raw[:, pair, :].T
    scales = [
        size ** (-0.5) * 1.4426950408889634
        for size in (DK_A + rope_width, pair_width - DK_A + rope_width)
    ]
    splits = ((slice(0, 128), slice(0, DV_A)), (slice(128, None), slice(DV_A, pair_width)))

    def block(index, first):
        source = own if first else held.at[index]
        compressed = source[:, :width]
        rope = source[:, width:]
        for pair in range(pairs):
            rows = jnp.dot(compressed, wk[pair], preferred_element_type=jnp.float32).astype(low)
            kx[pair, :, :128] = merge(rows[:, :128], rope)
            kx[pair, :, 128:256] = merge(rope, rows[:, :128])
            kx[pair, :, 256:] = rows[:, 128:]
            vt[pair] = lax.dot_general(
                wvt[pair], compressed, NT, preferred_element_type=jnp.float32
            ).astype(low)
        for pair in range(pairs):
            for group, (span, part) in enumerate(splits):
                head = pair * 2 + group
                scores = lax.dot_general(
                    kx[pair, :, span], qx[pair, :, span], NT, preferred_element_type=jnp.float32
                )
                if first:
                    row = lax.broadcasted_iota(jnp.int32, (tokens, tokens), 0)
                    column = lax.broadcasted_iota(jnp.int32, (tokens, tokens), 1)
                    scores = jnp.where(row <= column, scores, floor_score)
                    top = jnp.max(scores, axis=0, keepdims=True)
                else:
                    old = tops[head]
                    top = jnp.maximum(old, jnp.max(scores, axis=0, keepdims=True))
                    factor = jnp.exp2((old - top) * scales[group])
                weights = jnp.exp2((scores - top) * scales[group])
                total = jnp.sum(weights, axis=0, keepdims=True)
                update = jnp.dot(
                    vt[pair, part], weights.astype(low), preferred_element_type=jnp.float32
                )
                tops[head] = top
                if first:
                    sums[head] = total
                    acc[pair, part] = update
                else:
                    sums[head] = sums[head] * factor + total
                    acc[pair, part] = acc[pair, part] * factor + update

    block(me, True)

    def step(i, unused):
        index = me - 1 - i
        incoming(index).wait_recv()
        forward(index).start()
        forwarded(index).wait_recv()
        block(index, False)
        return unused

    lax.fori_loop(0, me, step, 0)
    for pair in range(pairs):
        for group, (span, part) in enumerate(splits):
            acc[pair, part] = acc[pair, part] / sums[pair * 2 + group]
        attention[:, pair * pair_width : (pair + 1) * pair_width] = acc[pair].T.astype(low)

    row_count, model = out_ref.shape
    middle = model // 256 * 128
    parts = (slice(0, middle), slice(middle, model))

    def swap(place, part):
        return remote(
            partial.at[place * 2 + 1 - core, :, parts[part]],
            partner_in.at[place, :, parts[part]],
            psend.at[place, part],
            precv.at[place, part],
            partner,
        )

    def pass_on(place, part, arrivals, sems, target):
        return remote(
            stage.at[place, :, parts[part]],
            arrivals.at[place, :, parts[part]],
            zsend.at[place, part],
            sems.at[place, part],
            target,
        )

    def up(place, part):
        return pass_on(place, part, up_in, urecv, above)

    def down(place, part):
        return pass_on(place, part, down_in, drecv, below)

    def pair_sum(place, part):
        swap(place, part).wait_recv()
        kept = partial[place * 2 + core, :, parts[part]].astype(jnp.float32)
        return kept + partner_in[place, :, parts[part]].astype(jnp.float32)

    def project(n, unused):
        turnabout = lax.rem(n, 2)
        place = turnabout * (n // 2) + (1 - turnabout) * (depth - 1 - n // 2)
        rows = pl.ds(pl.multiple_of(place * 2 * row_count, 2 * row_count), 2 * row_count)
        inputs = attention[rows]
        for part in range(2):
            mixed = jnp.dot(inputs, wo[:, parts[part]], preferred_element_type=jnp.float32)
            mixed = mixed.astype(low).reshape(2, row_count, mixed.shape[1])
            partial[pl.ds(place * 2, 2), :, parts[part]] = mixed
            swap(place, part).start()
        return unused

    lax.fori_loop(0, depth, project, 0)

    for j in range(depth - 1):
        high, deep = depth - 1 + z - j, j + z + 1 - depth
        for part in range(2):
            span = parts[part]

            @pl.when(z <= j)
            def _():
                stage[high, :, span] = pair_sum(high, part).astype(low)

                @pl.when(has_below)
                def _():
                    up(high, part).wait_recv()
                    stage[high, :, span] = (
                        stage[high, :, span].astype(jnp.float32)
                        + up_in[high, :, span].astype(jnp.float32)
                    ).astype(low)

                up(high, part).start()

            @pl.when(deep >= 0)
            def _():
                stage[deep, :, span] = pair_sum(deep, part).astype(low)

                @pl.when(has_above)
                def _():
                    down(deep, part).wait_recv()
                    stage[deep, :, span] = (
                        stage[deep, :, span].astype(jnp.float32)
                        + down_in[deep, :, span].astype(jnp.float32)
                    ).astype(low)

                down(deep, part).start()

    for part in range(2):
        span = parts[part]
        out_ref[:, span] = pair_sum(z, part)

        @pl.when(has_below)
        def _():
            up(z, part).wait_recv()
            out_ref[:, span] += up_in[z, :, span].astype(jnp.float32)

        @pl.when(has_above)
        def _():
            down(z, part).wait_recv()
            out_ref[:, span] += down_in[z, :, span].astype(jnp.float32)

    for place in range(sp_count):

        @pl.when(place < me)
        def _():
            forward(place).wait_send()

        @pl.when(place > me)
        def _():
            outgoing(place).wait_send()

    for place in range(depth):
        for part in range(2):
            swap(place, part).wait_send()

            @pl.when(place > z)
            def _():
                up(place, part).wait_send()

            @pl.when(place < z)
            def _():
                down(place, part).wait_send()


def attend(
    latent,
    latent_gain,
    key_rope,
    queries,
    query_rope,
    cosine,
    sine,
    key_weight,
    value_weight,
    out_weight,
    sp_count,
    tp_count,
    identity,
):
    tokens, latent_width = latent.shape
    pairs, pair_width = queries.shape[1:]
    rope_width = key_rope.shape[1]
    model = out_weight.shape[1]
    low = latent.dtype
    row_count = tokens // tp_count
    depth = tp_count // 2
    dma = pltpu.SemaphoreType.DMA
    vmem = pltpu.VMEM
    f32 = jnp.float32
    padded = pair_width + 128
    anywhere = pl.BlockSpec(memory_space=pl.ANY)
    block = vmem((depth, row_count, model), low)
    return pl.pallas_call(
        functools.partial(attend_kernel, rope_width, sp_count, tp_count),
        out_shape=jax.ShapeDtypeStruct((row_count, model), f32),
        in_specs=[anywhere, VM, VM, anywhere, VM, VM, VM, anywhere, anywhere, anywhere],
        out_specs=VM,
        scratch_shapes=[
            vmem(latent.shape, low),
            vmem(queries.shape, low),
            vmem(key_weight.shape, low),
            vmem(value_weight.shape, low),
            vmem(out_weight.shape, low),
            vmem((tokens, latent_width + 128), low),
            vmem((sp_count, tokens, latent_width + 128), low),
            vmem((pairs, tokens, padded), low),
            vmem((pairs, latent_width, pair_width), low),
            vmem((pairs, pair_width, latent_width), low),
            vmem((pairs, tokens, padded), low),
            vmem((pairs, pair_width, tokens), low),
            vmem((2 * pairs, 1, tokens), f32),
            vmem((2 * pairs, 1, tokens), f32),
            vmem((pairs, pair_width, tokens), f32),
            vmem((tokens, pairs * pair_width), low),
            vmem((tp_count, row_count, model), low),
            block,
            block,
            block,
            block,
            dma((5,)),
            dma((sp_count,)),
            dma((sp_count, 2)),
            dma((sp_count,)),
            dma((depth, 2)),
            dma((depth, 2)),
            dma((depth, 2)),
            dma((depth, 2)),
            dma((depth, 2)),
        ],
        compiler_params=pltpu.CompilerParams(
            collective_id=identity, has_side_effects=True, vmem_limit_bytes=60 * 1024 * 1024
        ),
    )(
        latent,
        latent_gain[None, :],
        key_rope.T,
        queries,
        query_rope.transpose(1, 2, 0),
        cosine,
        sine,
        key_weight,
        value_weight,
        out_weight,
    )


def local(
    residual,
    queries,
    query_rope,
    latent,
    key_rope,
    latent_gain,
    key_weight,
    value_weight,
    out_weight,
    norm_gain,
    routes,
    group_gate,
    expert_share,
    gate_weight,
    up_weight,
    down_weight,
):
    tokens = queries.shape[0]
    pair_dev = queries.shape[1]
    sp_count = lax.axis_size("sp")
    tp_count = lax.axis_size("tp")
    row_count = tokens // tp_count
    rope_width = key_rope.shape[1]
    low = jnp.bfloat16

    first_place = lax.axis_index("sp") * tokens
    places = (first_place + jnp.arange(tokens, dtype=jnp.int32)).astype(jnp.float32)
    cosine, sine = angle_tables(places, rope_width)
    head_total = attend(
        latent,
        latent_gain,
        key_rope,
        queries,
        query_rope,
        cosine,
        sine,
        key_weight,
        value_weight,
        out_weight.reshape(-1, residual.shape[1]),
        sp_count,
        tp_count,
        0,
    )
    routes, group_gate, expert_share, head_total = lax.optimization_barrier(
        (routes, group_gate, expert_share, head_total)
    )
    experts_dev = gate_weight.shape[0]
    experts_all = experts_dev * sp_count
    top_count = routes.shape[1]
    depth = tp_count // 2
    capacity = max(2, 3 * row_count * top_count // (2 * experts_all))
    slots = experts_dev * capacity
    if experts_all // GROUPS == experts_dev == top_count:
        slots = capacity
    slots = -(-slots // 8) * 8
    tp = lax.axis_index("tp")
    own = lax.dynamic_slice_in_dim(routes, tp * row_count, row_count, 0)
    route_weight = group_gate[:, None] * expert_share / jnp.sum(expert_share, axis=1, keepdims=True)
    expert_ids = jnp.arange(experts_all, dtype=jnp.int32)
    named = own[:, :, None] == expert_ids[None, None, :]
    table = jnp.sum(jnp.where(named, route_weight[:, :, None], 0.0), axis=1)
    weight_high = table.astype(low)
    weight_low = (table - weight_high.astype(jnp.float32)).astype(low)
    extra = jnp.concatenate([weight_high, weight_low], axis=1)
    extra = jnp.pad(extra, ((0, 0), (0, 128 - extra.shape[1])))

    column = lax.dynamic_index_in_dim(
        routes.reshape(depth, 2, row_count, top_count), lax.rem(tp, 2), 1, keepdims=False
    )
    goal = column // experts_dev
    member = jnp.any(goal[:, :, :, None] == jnp.arange(sp_count, dtype=jnp.int32), axis=2)
    row = jnp.arange(row_count, dtype=jnp.int32)
    earlier = (row[:, None] > row[None, :]).astype(low)
    member = member.astype(low)
    rank = jnp.einsum("rq,zqs->zsr", earlier, member, preferred_element_type=jnp.float32)
    rank = jnp.where(jnp.swapaxes(member, 1, 2) > 0, rank.astype(jnp.int32), -1)
    return moe(
        head_total,
        residual,
        norm_gain,
        extra,
        rank,
        slots,
        gate_weight,
        up_weight,
        down_weight,
        sp_count,
        tp_count,
        3,
    )


def solution(mesh):
    return jax.shard_map(
        local,
        mesh=mesh,
        in_specs=(
            P(("sp", "tp"), None),
            P("sp", "tp", None),
            P("sp", "tp", None),
            P("sp", None),
            P("sp", None),
            P(),
            P(None, "tp", None),
            P(None, "tp", None),
            P("tp", None, None),
            P(),
            P("sp", None),
            P(("sp", "tp")),
            P(("sp", "tp"), None),
            P("sp", None, "tp"),
            P("sp", None, "tp"),
            P("sp", "tp", None),
        ),
        out_specs=P(("sp", "tp"), None),
        check_vma=False,
    )
```

```python
import functools

import jax
import jax.numpy as jnp
from jax import lax
from jax.experimental import pallas as pl
from jax.experimental.pallas import tpu as pltpu
from jax.sharding import PartitionSpec as P

DK_A = 64
DV_A = 64
GROUPS = 4

rope_base = 10000.0
epsilon = 1e-06
floor_score = -1e30
MESH = pl.DeviceIdType.MESH
VM = pl.BlockSpec(memory_space=pltpu.VMEM)


def angle_tables(places, rope_width):
    steps = jnp.arange(rope_width // 2, dtype=jnp.int32)
    frequencies = rope_base ** (-(2 * steps).astype(jnp.float32) / rope_width)
    angles = places[None, :] * frequencies[:, None]
    return (jnp.cos(angles), jnp.sin(angles))


def rms_scale(values, gain_vector):
    values = values.astype(jnp.float32)
    inverse = lax.rsqrt(jnp.mean(values * values, axis=-1, keepdims=True) + epsilon)
    return values * inverse * gain_vector


def remote(src, dst, send, recv, target):
    return pltpu.make_async_remote_copy(
        src_ref=src,
        dst_ref=dst,
        send_sem=send,
        recv_sem=recv,
        device_id=target,
        device_id_type=MESH,
    )


def greet_some(targets):
    barrier = pltpu.get_barrier_semaphore()
    count = 0
    for here, target in targets:

        @pl.when(here)
        def _():
            pl.semaphore_signal(barrier, inc=1, device_id=target, device_id_type=MESH)

        count = count + jnp.where(here, 1, 0)
    return lambda: pl.semaphore_wait(barrier, count)


def line(tp_count):
    sp = lax.axis_index("sp")
    tp = lax.axis_index("tp")
    core = lax.rem(tp, 2)
    z = lax.div(tp, 2)
    depth = tp_count // 2
    partner = (sp, tp + 1 - 2 * core)
    return sp, core, z, depth, partner, (sp, tp + 2), (sp, tp - 2), z < depth - 1, z > 0


def moe_kernel(
    sp_count,
    tp_count,
    spare,
    heads_ref,
    residual_ref,
    norm_gain_ref,
    extra_ref,
    rank_ref,
    gate_ref,
    up_ref,
    down_ref,
    out_ref,
    own,
    token_rows,
    held,
    picked,
    rows,
    gate,
    up,
    down,
    result,
    result_spare,
    swapped,
    swapped_spare,
    summed,
    back,
    mixed,
    stage,
    up_in,
    down_in,
    usend,
    dsend,
    recv,
    ssend,
    srecv,
    fsend,
    frecv,
    wsend,
    wrecv,
    vsend,
    vrecv,
    rsend,
    rrecv,
    zsend,
    urecv,
    drecv,
    wsem,
):
    me, core, z, depth, partner, above, below, has_above, has_below = line(tp_count)
    tp = lax.axis_index("tp")
    experts = gate_ref.shape[0]
    model = gate_ref.shape[1]
    tokens, wide = own.shape
    slots = rows.shape[3]
    low = own.dtype
    middle = model // 2
    segment = middle * spare // slots
    sent = middle + segment
    line_parts = (slice(0, middle), slice(middle, wide))
    parts = (slice(0, middle), slice(middle, model))
    gather_parts = (slice(0, sent), slice(sent, rows.shape[4]))
    return_parts = (slice(0, sent), slice(sent, 2 * sent))

    def fold_matrix(k, count, flat):
        full, few = count * slots, count * spare
        shape = (full, few) if flat else (few, full)
        row = lax.broadcasted_iota(jnp.int32, shape, 0 if flat else 1)
        column = lax.broadcasted_iota(jnp.int32, shape, 1 if flat else 0)
        place = row & (slots - 1)
        low_bits = spare.bit_length() - 1
        owner = (row >> (slots.bit_length() - 1)) << low_bits
        here = ((place >> low_bits) == k) & (column == owner + (row & (spare - 1)))
        return jnp.where(here, 1.0, 0.0).astype(low)

    def fold(extra_rows):
        count = extra_rows.shape[0] // spare
        total = None
        for k in range(slots // spare):
            piece = extra_rows[:, k * segment : (k + 1) * segment]
            matrix = fold_matrix(k, count, True)
            term = jnp.dot(matrix, piece, preferred_element_type=jnp.float32)
            total = term if k == 0 else total + term
        return total.astype(low)

    def unfold(folded):
        count = folded.shape[0] // slots
        pieces = [
            jnp.dot(fold_matrix(k, count, False), folded, preferred_element_type=jnp.float32)
            for k in range(slots // spare)
        ]
        return jnp.concatenate(pieces, axis=1).astype(low)

    def one_hot(place, start, height, limit):
        row = lax.broadcasted_iota(jnp.int32, (height, tokens), 0)
        wanted = jnp.where(row < limit, row + start, -2)
        pieces = [
            jnp.where(rank_ref[place, source : source + 1] == wanted, 1.0, 0.0)
            for source in range(sp_count)
        ]
        return jnp.concatenate(pieces, axis=0)

    def spare_hot(place):
        full = one_hot(place, slots, slots, spare)
        matrix = fold_matrix(0, sp_count, False)
        return jnp.dot(matrix, full.astype(low), preferred_element_type=jnp.float32)

    others = [lax.rem(me + k, sp_count) for k in reversed(range(1, sp_count))]
    loads = [
        pltpu.make_async_copy(source, target, wsem.at[i])
        for i, (source, target) in enumerate(((gate_ref, gate), (up_ref, up), (down_ref, down)))
    ]
    met = greet_some(
        [(True, partner), (has_above, above), (has_below, below)]
        + [(True, (other, tp)) for other in others]
    )
    for load in loads:
        load.start()
    total = residual_ref[...].astype(jnp.float32) + heads_ref[...]
    token_rows[...] = total
    own[:, :model] = rms_scale(total, norm_gain_ref[...]).astype(low)
    own[:, model:] = extra_ref[...]
    met()

    def move(place, sems, part, target, source=None):
        source = held.at[place] if source is None else source
        return remote(
            source.at[:, line_parts[part]],
            held.at[place, :, line_parts[part]],
            sems.at[place, part],
            recv.at[place, part],
            target,
        )

    for part in range(2):

        @pl.when(has_above)
        def _():
            move(z, usend, part, above, own).start()

        @pl.when(has_below)
        def _():
            move(z, dsend, part, below, own).start()

    held[z] = own[...]
    def send_to(source, target, sends, recvs, place, part, mark, arrive, device):
        return remote(
            source, target, sends.at[place, mark, part], recvs.at[place, arrive, part], device
        )

    def spread(place, part, other, arrive=None):
        arrive = me if arrive is None else arrive
        span = gather_parts[part]
        return send_to(
            picked.at[place, other, :, span],
            rows.at[place, core, arrive, :, span],
            ssend,
            srecv,
            place,
            part,
            other,
            arrive,
            (other, tp),
        )

    def share(place, part, source, own_rows=False):
        span = gather_parts[part]
        target = rows.at[place, core, source, :, span]
        start = picked.at[place, source, :, span] if own_rows else target
        return send_to(start, target, fsend, frecv, place, part, source, source, partner)

    def shared(place, part, source):
        target = rows.at[place, 1 - core, source, :, gather_parts[part]]
        return send_to(target, target, fsend, frecv, place, part, source, source, partner)

    def swap(place, part):
        return remote(
            result.at[place, 1 - core, :, :, parts[part]],
            swapped.at[place, :, :, parts[part]],
            wsend.at[place, part],
            wrecv.at[place, part],
            partner,
        )

    def swap_spare(place, part):
        return remote(
            result_spare.at[place, 1 - core, :, parts[part]],
            swapped_spare.at[place, :, parts[part]],
            vsend.at[place, part],
            vrecv.at[place, part],
            partner,
        )

    def give(place, part, other, arrive=None):
        arrive = me if arrive is None else arrive
        span = return_parts[part]
        return send_to(
            summed.at[place, other, :, span],
            back.at[place, arrive, :, span],
            rsend,
            rrecv,
            place,
            part,
            other,
            arrive,
            (other, tp),
        )

    def pass_on(place, part, arrivals, sems, target):
        return remote(
            stage.at[place, :, parts[part]],
            arrivals.at[place, :, parts[part]],
            zsend.at[place, part],
            sems.at[place, part],
            target,
        )

    def rise(place, part):
        return pass_on(place, part, up_in, urecv, above)

    def fall(place, part):
        return pass_on(place, part, down_in, drecv, below)

    def take(k, part):
        lower, upper = z - k, z + k

        @pl.when((k > 0) & (lower >= 0))
        def _():
            move(lower, usend, part, below).wait_recv()

            @pl.when(has_above)
            def _():
                move(lower, usend, part, above).start()

        @pl.when((k > 0) & (upper < depth))
        def _():
            move(upper, dsend, part, above).wait_recv()

            @pl.when(has_below)
            def _():
                move(upper, dsend, part, below).start()

    def choose(place, part):
        span = parts[part]
        base = gather_parts[part].start
        inputs = held[place, :, span]
        pick = one_hot(place, 0, slots, slots).astype(low)

        def keep(value, start):
            width = value.shape[1]
            picked[place, :, :, start : start + width] = value.astype(low).reshape(
                sp_count, slots, width
            )

        keep(jnp.dot(pick, inputs, preferred_element_type=jnp.float32), base)
        if spare:
            few = spare_hot(place).astype(low)
            extra_rows = jnp.dot(few, inputs, preferred_element_type=jnp.float32).astype(low)
            keep(fold(extra_rows), base + middle)
        if part == 1:
            tail = held[place, :, model:]
            chosen = jnp.dot(pick, tail, preferred_element_type=jnp.float32)
            if spare:
                full = one_hot(place, slots, slots, spare).astype(low)
                second = jnp.dot(full, tail, preferred_element_type=jnp.float32)
                lane = lax.broadcasted_iota(jnp.int32, chosen.shape, 1)
                chosen = jnp.where(lane < 64, chosen, second)
            keep(chosen, 2 * sent)
        for other in others:
            spread(place, part, other).start()
        share(place, part, me, True).start()
        rows[place, core, me, :, gather_parts[part]] = picked[place, me, :, gather_parts[part]]

    def relay(place, part):
        for other in others:
            spread(place, part, other, other).wait_recv()
            share(place, part, other).start()

    def compute(place):
        for part in range(2):
            for source in range(sp_count):
                shared(place, part, source).wait_recv()
        count = 2 * sp_count
        full = count * slots

        def stretch(start, width):
            return rows[place, :, :, :, start : start + width].reshape(full, width)

        inputs = []
        for part in range(2):
            x = stretch(part * sent, middle)
            if spare:
                few = unfold(stretch(part * sent + middle, segment))
                x = jnp.concatenate([x, few], axis=0)
            inputs.append(x)
        tail = stretch(2 * sent, 128)
        tails = [(tail.astype(jnp.float32), 0)]
        if spare:
            first = fold_matrix(0, count, False)
            tails.append((jnp.dot(first, tail, preferred_element_type=jnp.float32), 64))

        def scale_of(values, index):
            lane = lax.broadcasted_iota(jnp.int32, values.shape, 1)
            here = (lane == index) | (lane == index + experts * sp_count)
            return jnp.sum(jnp.where(here, values, 0.0), axis=1, keepdims=True)

        def expand(weight):
            return jnp.dot(
                inputs[0], weight[:middle], preferred_element_type=jnp.float32
            ) + jnp.dot(inputs[1], weight[middle:], preferred_element_type=jnp.float32)

        hidden = []
        for e in range(experts):
            index = me * experts + e
            scale = [scale_of(values, index + start) for values, start in tails]
            scale = jnp.concatenate(scale, axis=0) if spare else scale[0]
            gate_out = expand(gate.at[e])
            up_out = expand(up.at[e])
            hidden.append((jax.nn.silu(gate_out) * up_out * scale).astype(low))
        for part in range(2):
            span = parts[part]
            total = jnp.dot(hidden[0], down[0, :, span], preferred_element_type=jnp.float32)
            for e in range(1, experts):
                total += jnp.dot(hidden[e], down[e, :, span], preferred_element_type=jnp.float32)
            total = total.astype(low)
            result[place, :, :, :, span] = total[:full].reshape(2, sp_count, slots, middle)
            if spare:
                result_spare[place, :, :, span] = total[full:].reshape(
                    2, sp_count * spare, middle
                )
                swap_spare(place, part).start()
            swap(place, part).start()

    def settle(place, part):
        span = parts[part]
        base = return_parts[part].start
        swap(place, part).wait_recv()
        kept = result[place, core, :, :, span].astype(jnp.float32)
        both = kept + swapped[place, :, :, span].astype(jnp.float32)
        summed[place, :, :, base : base + middle] = both.astype(low)
        if spare:
            swap_spare(place, part).wait_recv()
            kept = result_spare[place, core, :, span].astype(jnp.float32)
            both = kept + swapped_spare[place, :, span].astype(jnp.float32)
            summed[place, :, :, base + middle : base + sent] = fold(both.astype(low)).reshape(
                sp_count, slots, segment
            )
        for other in others:
            give(place, part, other).start()
        back[place, me, :, base : base + sent] = summed[place, me, :, base : base + sent]

    def combine(place, part):
        span = parts[part]
        base = return_parts[part].start
        for other in others:
            give(place, part, other, other).wait_recv()

        def gathered(start, width):
            return back[place, :, :, start : start + width].reshape(sp_count * slots, width)

        total = jnp.dot(
            one_hot(place, 0, slots, slots).T.astype(low),
            gathered(base, middle),
            preferred_element_type=jnp.float32,
        )
        if spare:
            total += jnp.dot(
                spare_hot(place).T.astype(low),
                unfold(gathered(base + middle, segment)),
                preferred_element_type=jnp.float32,
            )
        mixed[place, :, span] = total

        @pl.when((place > z) & (z == 0))
        def _():
            stage[place, :, span] = mixed[place, :, span].astype(low)
            rise(place, part).start()

        @pl.when((place < z) & (z == depth - 1))
        def _():
            stage[place, :, span] = mixed[place, :, span].astype(low)
            fall(place, part).start()

    def at(k, action):
        def one(side, unused):
            place = z + (1 - 2 * side) * k

            @pl.when((place >= 0) & (place < depth) & ((k > 0) | (side == 0)) & (k >= 0))
            def _():
                action(place)

            return unused

        lax.fori_loop(0, 2, one, 0)

    def step(t, unused):
        @pl.when(t < depth)
        def _():
            for part in range(2):
                take(t, part)
                at(t, lambda place: choose(place, part))

        @pl.when(t == 1)
        def _():
            for load in loads:
                load.wait()

        for action, late in ((relay, 1), (settle, 2), (combine, 3)):
            for part in range(2):
                at(t - late, lambda place: action(place, part))
        at(t - 1, compute)
        return unused

    lax.fori_loop(0, depth + 3, step, 0)

    def hop(key, unused):
        high = key - z
        deep = 2 * depth - 2 - key - z
        for part in range(2):
            span = parts[part]

            @pl.when((high > z) & (high < depth) & has_below)
            def _():
                rise(high, part).wait_recv()
                stage[high, :, span] = (
                    mixed[high, :, span] + up_in[high, :, span].astype(jnp.float32)
                ).astype(low)
                rise(high, part).start()

            @pl.when((deep >= 0) & (deep < z) & has_above)
            def _():
                fall(deep, part).wait_recv()
                stage[deep, :, span] = (
                    mixed[deep, :, span] + down_in[deep, :, span].astype(jnp.float32)
                ).astype(low)
                fall(deep, part).start()

        return unused

    lax.fori_loop(1, 2 * depth - 2, hop, 0)
    for part in range(2):
        span = parts[part]
        token_rows[:, span] += mixed[z, :, span]

        @pl.when(has_below)
        def _():
            rise(z, part).wait_recv()
            token_rows[:, span] += up_in[z, :, span].astype(jnp.float32)

        @pl.when(has_above)
        def _():
            fall(z, part).wait_recv()
            token_rows[:, span] += down_in[z, :, span].astype(jnp.float32)

        out_ref[:, span] = token_rows[:, span].astype(low)

    def finish(place, unused):
        for part in range(2):

            @pl.when(has_above & (place <= z))
            def _():
                move(place, usend, part, above).wait_send()

            @pl.when(has_below & (place >= z))
            def _():
                move(place, dsend, part, below).wait_send()

            @pl.when(place > z)
            def _():
                rise(place, part).wait_send()

            @pl.when(place < z)
            def _():
                fall(place, part).wait_send()

            for other in others:
                spread(place, part, other).wait_send()
                share(place, part, other).wait_send()
                give(place, part, other).wait_send()
            share(place, part, me, True).wait_send()
            swap(place, part).wait_send()
            if spare:
                swap_spare(place, part).wait_send()
        return unused

    lax.fori_loop(0, depth, finish, 0)


def moe(
    heads,
    residual,
    norm_gain,
    extra,
    rank,
    slots,
    gate_weight,
    up_weight,
    down_weight,
    sp_count,
    tp_count,
    identity,
):
    dma = pltpu.SemaphoreType.DMA
    depth = tp_count // 2
    tokens, model = residual.shape
    wide = model + extra.shape[1]
    low = residual.dtype
    spare = slots % 8
    fits = spare in (1, 2, 4) and slots - spare in (8, 16, 32, 64)
    if fits and model // 2 * spare // (slots - spare) % 128 == 0:
        slots = slots - spare
    else:
        spare = 0
        slots = -(-slots // 8) * 8
    sent = model // 2 * (slots + spare) // slots
    anywhere = pl.BlockSpec(memory_space=pl.ANY)
    each = dma((depth, sp_count, 2))
    two = dma((depth, 2))
    block = pltpu.VMEM((depth, tokens, model), low)
    group = pltpu.VMEM((depth, sp_count, slots, model), low)
    carried = pltpu.VMEM((depth, sp_count, slots, 2 * sent), low)
    few = max(spare * sp_count, 8)
    return pl.pallas_call(
        functools.partial(moe_kernel, sp_count, tp_count, spare),
        out_shape=jax.ShapeDtypeStruct((tokens, model), low),
        in_specs=[VM, VM, VM, VM, VM, anywhere, anywhere, anywhere],
        out_specs=VM,
        scratch_shapes=[
            pltpu.VMEM((tokens, wide), low),
            pltpu.VMEM((tokens, model), jnp.float32),
            pltpu.VMEM((depth, tokens, wide), low),
            pltpu.VMEM((depth, sp_count, slots, 2 * sent + 128), low),
            pltpu.VMEM((depth, 2, sp_count, slots, 2 * sent + 128), low),
            pltpu.VMEM(gate_weight.shape, gate_weight.dtype),
            pltpu.VMEM(up_weight.shape, up_weight.dtype),
            pltpu.VMEM(down_weight.shape, down_weight.dtype),
            pltpu.VMEM((depth, 2, sp_count, slots, model), low),
            pltpu.VMEM((depth, 2, few, model), low),
            group,
            pltpu.VMEM((depth, few, model), low),
            carried,
            carried,
            pltpu.VMEM((depth, tokens, model), jnp.float32),
            block,
            block,
            block,
            two,
            two,
            two,
            each,
            each,
            each,
            each,
            two,
            two,
            two,
            two,
            each,
            each,
            two,
            two,
            two,
            dma((3,)),
        ],
        compiler_params=pltpu.CompilerParams(
            collective_id=identity, has_side_effects=True, vmem_limit_bytes=60 * 1024 * 1024
        ),
    )(heads, residual, norm_gain[None, :], extra, rank, gate_weight, up_weight, down_weight)


NT = (((1,), (1,)), ((), ()))


def attend_kernel(
    rope_width,
    sp_count,
    tp_count,
    latent_ref,
    gain_ref,
    key_rope_ref,
    q_ref,
    q_rope_ref,
    cos_ref,
    sin_ref,
    wk_ref,
    wv_ref,
    wo_ref,
    out_ref,
    latent,
    queries,
    wk_raw,
    wv_raw,
    wo,
    own,
    held,
    qx,
    wk,
    wvt,
    kx,
    vt,
    tops,
    sums,
    acc,
    attention,
    partial,
    partner_in,
    stage,
    up_in,
    down_in,
    wsem,
    send,
    recv,
    fsend,
    psend,
    precv,
    zsend,
    urecv,
    drecv,
):
    me, core, z, depth, partner, above, below, has_above, has_below = line(tp_count)
    tp = lax.axis_index("tp")
    tokens, width = latent.shape
    pairs, pair_width = queries.shape[1:]
    half = tokens // 2
    low = own.dtype
    loads = [
        pltpu.make_async_copy(source, target, wsem.at[i])
        for i, (source, target) in enumerate(
            (
                (latent_ref, latent),
                (q_ref, queries),
                (wk_ref, wk_raw),
                (wv_ref, wv_raw),
                (wo_ref, wo),
            )
        )
    ]
    loads[0].start()
    met = greet_some(
        [(True, partner), (has_above, above), (has_below, below)]
        + [(True, (lax.rem(me + k, sp_count), tp)) for k in range(1, sp_count)]
    )
    mine = pl.ds(pl.multiple_of(core * half, half), half)
    other = pl.ds(pl.multiple_of((1 - core) * half, half), half)

    def outgoing(to):
        return remote(own.at[mine], held.at[me, mine], send.at[to], recv.at[me, core], (to, tp))

    def incoming(source):
        return remote(
            own.at[mine], held.at[source, mine], send.at[source], recv.at[source, core], partner
        )

    def forward(source):
        return remote(
            held.at[source, mine],
            held.at[source, mine],
            fsend.at[source],
            recv.at[source, core],
            partner,
        )

    def forwarded(source):
        return remote(
            held.at[source, other],
            held.at[source, other],
            fsend.at[source],
            recv.at[source, 1 - core],
            partner,
        )

    turn = rope_width // 2
    cosine, sine = cos_ref[...], sin_ref[...]

    def rotate(upper, lower):
        return upper * cosine - lower * sine, lower * cosine + upper * sine

    raw = key_rope_ref[...].astype(jnp.float32)
    rotated = list(rotate(raw[:turn], raw[turn:]))
    own[:, width:] = jnp.concatenate(rotated * (128 // rope_width), axis=0).T.astype(low)
    loads[0].wait()
    for load in loads[1:]:
        load.start()
    values = latent[...].astype(jnp.float32)
    inverse = lax.rsqrt(jnp.mean(values * values, axis=-1, keepdims=True) + epsilon)
    own[:, :width] = (values * inverse * gain_ref[...]).astype(low)

    met()
    for to in reversed(range(sp_count)):

        @pl.when(to > me)
        def _():
            outgoing(to).start()

    def merge(one, two):
        lane = lax.broadcasted_iota(jnp.int32, one.shape, 1)
        return jnp.where(lane < DK_A, one, two)

    for load in loads[1:4]:
        load.wait()
    gap = jnp.zeros((DK_A - rope_width, tokens), jnp.float32)
    for pair in range(pairs):
        rope = q_rope_ref[pair].astype(jnp.float32)
        first = list(rotate(rope[:turn], rope[turn:rope_width]))
        second = list(rotate(rope[rope_width : rope_width + turn], rope[rope_width + turn :]))
        turned = jnp.concatenate(second + [gap] + first + [gap], axis=0).T.astype(low)
        qx[pair, :, 128:] = queries[:, pair, :]
        query = qx[pair, :, 128:256]
        qx[pair, :, :128] = merge(query, turned)
        qx[pair, :, 128:256] = merge(turned, query)
        wk[pair] = wk_raw[:, pair, :]
        wvt[pair] = wv_raw[:, pair, :].T
    scales = [
        size ** (-0.5) * 1.4426950408889634
        for size in (DK_A + rope_width, pair_width - DK_A + rope_width)
    ]
    splits = ((slice(0, 128), slice(0, DV_A)), (slice(128, None), slice(DV_A, pair_width)))

    def block(index, first):
        source = own if first else held.at[index]
        compressed = source[:, :width]
        rope = source[:, width:]
        for pair in range(pairs):
            rows = jnp.dot(compressed, wk[pair], preferred_element_type=jnp.float32).astype(low)
            kx[pair, :, :128] = merge(rows[:, :128], rope)
            kx[pair, :, 128:256] = merge(rope, rows[:, :128])
            kx[pair, :, 256:] = rows[:, 128:]
            vt[pair] = lax.dot_general(
                wvt[pair], compressed, NT, preferred_element_type=jnp.float32
            ).astype(low)
        for pair in range(pairs):
            for group, (span, part) in enumerate(splits):
                head = pair * 2 + group
                scores = lax.dot_general(
                    kx[pair, :, span], qx[pair, :, span], NT, preferred_element_type=jnp.float32
                )
                if first:
                    row = lax.broadcasted_iota(jnp.int32, (tokens, tokens), 0)
                    column = lax.broadcasted_iota(jnp.int32, (tokens, tokens), 1)
                    scores = jnp.where(row <= column, scores, floor_score)
                    top = jnp.max(scores, axis=0, keepdims=True)
                else:
                    old = tops[head]
                    top = jnp.maximum(old, jnp.max(scores, axis=0, keepdims=True))
                    factor = jnp.exp2((old - top) * scales[group])
                weights = jnp.exp2((scores - top) * scales[group])
                total = jnp.sum(weights, axis=0, keepdims=True)
                update = jnp.dot(
                    vt[pair, part], weights.astype(low), preferred_element_type=jnp.float32
                )
                tops[head] = top
                if first:
                    sums[head] = total
                    acc[pair, part] = update
                else:
                    sums[head] = sums[head] * factor + total
                    acc[pair, part] = acc[pair, part] * factor + update

    block(me, True)

    def step(i, unused):
        index = me - 1 - i
        incoming(index).wait_recv()
        forward(index).start()
        forwarded(index).wait_recv()
        block(index, False)
        return unused

    lax.fori_loop(0, me, step, 0)
    for pair in range(pairs):
        for group, (span, part) in enumerate(splits):
            acc[pair, part] = acc[pair, part] / sums[pair * 2 + group]
        attention[:, pair * pair_width : (pair + 1) * pair_width] = acc[pair].T.astype(low)

    row_count, model = out_ref.shape
    middle = model // 256 * 128
    parts = (slice(0, middle), slice(middle, model))

    def swap(place, part):
        return remote(
            partial.at[place * 2 + 1 - core, :, parts[part]],
            partner_in.at[place, :, parts[part]],
            psend.at[place, part],
            precv.at[place, part],
            partner,
        )

    def pass_on(place, part, arrivals, sems, target):
        return remote(
            stage.at[place, :, parts[part]],
            arrivals.at[place, :, parts[part]],
            zsend.at[place, part],
            sems.at[place, part],
            target,
        )

    def up(place, part):
        return pass_on(place, part, up_in, urecv, above)

    def down(place, part):
        return pass_on(place, part, down_in, drecv, below)

    def pair_sum(place, part):
        swap(place, part).wait_recv()
        kept = partial[place * 2 + core, :, parts[part]].astype(jnp.float32)
        return kept + partner_in[place, :, parts[part]].astype(jnp.float32)

    def project(n, unused):
        turnabout = lax.rem(n, 2)
        place = turnabout * (n // 2) + (1 - turnabout) * (depth - 1 - n // 2)
        rows = pl.ds(pl.multiple_of(place * 2 * row_count, 2 * row_count), 2 * row_count)
        inputs = attention[rows]
        for part in range(2):
            mixed = jnp.dot(inputs, wo[:, parts[part]], preferred_element_type=jnp.float32)
            mixed = mixed.astype(low).reshape(2, row_count, mixed.shape[1])
            partial[pl.ds(place * 2, 2), :, parts[part]] = mixed
            swap(place, part).start()
        return unused

    loads[4].wait()
    lax.fori_loop(0, depth, project, 0)

    for j in range(depth - 1):
        high, deep = depth - 1 + z - j, j + z + 1 - depth
        for part in range(2):
            span = parts[part]

            @pl.when(z <= j)
            def _():
                stage[high, :, span] = pair_sum(high, part).astype(low)

                @pl.when(has_below)
                def _():
                    up(high, part).wait_recv()
                    stage[high, :, span] = (
                        stage[high, :, span].astype(jnp.float32)
                        + up_in[high, :, span].astype(jnp.float32)
                    ).astype(low)

                up(high, part).start()

            @pl.when(deep >= 0)
            def _():
                stage[deep, :, span] = pair_sum(deep, part).astype(low)

                @pl.when(has_above)
                def _():
                    down(deep, part).wait_recv()
                    stage[deep, :, span] = (
                        stage[deep, :, span].astype(jnp.float32)
                        + down_in[deep, :, span].astype(jnp.float32)
                    ).astype(low)

                down(deep, part).start()

    for part in range(2):
        span = parts[part]
        out_ref[:, span] = pair_sum(z, part)

        @pl.when(has_below)
        def _():
            up(z, part).wait_recv()
            out_ref[:, span] += up_in[z, :, span].astype(jnp.float32)

        @pl.when(has_above)
        def _():
            down(z, part).wait_recv()
            out_ref[:, span] += down_in[z, :, span].astype(jnp.float32)

    for place in range(sp_count):

        @pl.when(place < me)
        def _():
            forward(place).wait_send()

        @pl.when(place > me)
        def _():
            outgoing(place).wait_send()

    for place in range(depth):
        for part in range(2):
            swap(place, part).wait_send()

            @pl.when(place > z)
            def _():
                up(place, part).wait_send()

            @pl.when(place < z)
            def _():
                down(place, part).wait_send()


def attend(
    latent,
    latent_gain,
    key_rope,
    queries,
    query_rope,
    cosine,
    sine,
    key_weight,
    value_weight,
    out_weight,
    sp_count,
    tp_count,
    identity,
):
    tokens, latent_width = latent.shape
    pairs, pair_width = queries.shape[1:]
    rope_width = key_rope.shape[1]
    model = out_weight.shape[1]
    low = latent.dtype
    row_count = tokens // tp_count
    depth = tp_count // 2
    dma = pltpu.SemaphoreType.DMA
    vmem = pltpu.VMEM
    f32 = jnp.float32
    padded = pair_width + 128
    anywhere = pl.BlockSpec(memory_space=pl.ANY)
    block = vmem((depth, row_count, model), low)
    return pl.pallas_call(
        functools.partial(attend_kernel, rope_width, sp_count, tp_count),
        out_shape=jax.ShapeDtypeStruct((row_count, model), f32),
        in_specs=[anywhere, VM, VM, anywhere, VM, VM, VM, anywhere, anywhere, anywhere],
        out_specs=VM,
        scratch_shapes=[
            vmem(latent.shape, low),
            vmem(queries.shape, low),
            vmem(key_weight.shape, low),
            vmem(value_weight.shape, low),
            vmem(out_weight.shape, low),
            vmem((tokens, latent_width + 128), low),
            vmem((sp_count, tokens, latent_width + 128), low),
            vmem((pairs, tokens, padded), low),
            vmem((pairs, latent_width, pair_width), low),
            vmem((pairs, pair_width, latent_width), low),
            vmem((pairs, tokens, padded), low),
            vmem((pairs, pair_width, tokens), low),
            vmem((2 * pairs, 1, tokens), f32),
            vmem((2 * pairs, 1, tokens), f32),
            vmem((pairs, pair_width, tokens), f32),
            vmem((tokens, pairs * pair_width), low),
            vmem((tp_count, row_count, model), low),
            block,
            block,
            block,
            block,
            dma((5,)),
            dma((sp_count,)),
            dma((sp_count, 2)),
            dma((sp_count,)),
            dma((depth, 2)),
            dma((depth, 2)),
            dma((depth, 2)),
            dma((depth, 2)),
            dma((depth, 2)),
        ],
        compiler_params=pltpu.CompilerParams(
            collective_id=identity, has_side_effects=True, vmem_limit_bytes=60 * 1024 * 1024
        ),
    )(
        latent,
        latent_gain[None, :],
        key_rope.T,
        queries,
        query_rope.transpose(1, 2, 0),
        cosine,
        sine,
        key_weight,
        value_weight,
        out_weight,
    )


def local(
    residual,
    queries,
    query_rope,
    latent,
    key_rope,
    latent_gain,
    key_weight,
    value_weight,
    out_weight,
    norm_gain,
    routes,
    group_gate,
    expert_share,
    gate_weight,
    up_weight,
    down_weight,
):
    tokens = queries.shape[0]
    pair_dev = queries.shape[1]
    sp_count = lax.axis_size("sp")
    tp_count = lax.axis_size("tp")
    row_count = tokens // tp_count
    rope_width = key_rope.shape[1]
    low = jnp.bfloat16

    first_place = lax.axis_index("sp") * tokens
    places = (first_place + jnp.arange(tokens, dtype=jnp.int32)).astype(jnp.float32)
    cosine, sine = angle_tables(places, rope_width)
    head_total = attend(
        latent,
        latent_gain,
        key_rope,
        queries,
        query_rope,
        cosine,
        sine,
        key_weight,
        value_weight,
        out_weight.reshape(-1, residual.shape[1]),
        sp_count,
        tp_count,
        0,
    )
    routes, group_gate, expert_share, head_total = lax.optimization_barrier(
        (routes, group_gate, expert_share, head_total)
    )
    experts_dev = gate_weight.shape[0]
    experts_all = experts_dev * sp_count
    top_count = routes.shape[1]
    depth = tp_count // 2
    capacity = max(2, 3 * row_count * top_count // (2 * experts_all))
    slots = experts_dev * capacity
    if experts_all // GROUPS == experts_dev == top_count:
        slots = capacity
    tp = lax.axis_index("tp")
    own = lax.dynamic_slice_in_dim(routes, tp * row_count, row_count, 0)
    route_weight = group_gate[:, None] * expert_share / jnp.sum(expert_share, axis=1, keepdims=True)
    expert_ids = jnp.arange(experts_all, dtype=jnp.int32)
    named = own[:, :, None] == expert_ids[None, None, :]
    table = jnp.sum(jnp.where(named, route_weight[:, :, None], 0.0), axis=1)
    weight_high = table.astype(low)
    weight_low = (table - weight_high.astype(jnp.float32)).astype(low)
    extra = jnp.concatenate([weight_high, weight_low], axis=1)
    extra = jnp.pad(extra, ((0, 0), (0, 64 - extra.shape[1])))
    extra = jnp.concatenate([extra, extra], axis=1)

    column = lax.dynamic_index_in_dim(
        routes.reshape(depth, 2, row_count, top_count), lax.rem(tp, 2), 1, keepdims=False
    )
    goal = column // experts_dev
    member = jnp.any(goal[:, :, :, None] == jnp.arange(sp_count, dtype=jnp.int32), axis=2)
    row = jnp.arange(row_count, dtype=jnp.int32)
    earlier = (row[:, None] > row[None, :]).astype(low)
    member = member.astype(low)
    rank = jnp.einsum("rq,zqs->zsr", earlier, member, preferred_element_type=jnp.float32)
    rank = jnp.where(jnp.swapaxes(member, 1, 2) > 0, rank.astype(jnp.int32), -1)
    return moe(
        head_total,
        residual,
        norm_gain,
        extra,
        rank,
        slots,
        gate_weight,
        up_weight,
        down_weight,
        sp_count,
        tp_count,
        3,
    )


def solution(mesh):
    return jax.shard_map(
        local,
        mesh=mesh,
        in_specs=(
            P(("sp", "tp"), None),
            P("sp", "tp", None),
            P("sp", "tp", None),
            P("sp", None),
            P("sp", None),
            P(),
            P(None, "tp", None),
            P(None, "tp", None),
            P("tp", None, None),
            P(),
            P("sp", None),
            P(("sp", "tp")),
            P(("sp", "tp"), None),
            P("sp", None, "tp"),
            P("sp", None, "tp"),
            P("sp", "tp", None),
        ),
        out_specs=P(("sp", "tp"), None),
        check_vma=False,
    )
```

```python
import functools

import jax
import jax.numpy as jnp
from jax import lax
from jax.experimental import pallas as pl
from jax.experimental.pallas import tpu as pltpu
from jax.sharding import PartitionSpec as P

DK_A = 64
DV_A = 64
GROUPS = 4

rope_base = 10000.0
epsilon = 1e-06
floor_score = -1e30
PIECES = 4
MESH = pl.DeviceIdType.MESH
VM = pl.BlockSpec(memory_space=pltpu.VMEM)


def angle_tables(places, rope_width):
    steps = jnp.arange(rope_width // 2, dtype=jnp.int32)
    frequencies = rope_base ** (-(2 * steps).astype(jnp.float32) / rope_width)
    angles = places[None, :] * frequencies[:, None]
    return (jnp.cos(angles), jnp.sin(angles))


def rms_scale(values, gain_vector):
    values = values.astype(jnp.float32)
    inverse = lax.rsqrt(jnp.mean(values * values, axis=-1, keepdims=True) + epsilon)
    return values * inverse * gain_vector


def remote(src, dst, send, recv, target):
    return pltpu.make_async_remote_copy(
        src_ref=src,
        dst_ref=dst,
        send_sem=send,
        recv_sem=recv,
        device_id=target,
        device_id_type=MESH,
    )


def grant(scratch, extra):
    total = 0
    for item in scratch:
        if item.memory_space == pltpu.VMEM:
            size = 1
            for width in item.shape[:-1]:
                size *= width
            total += size * max(item.shape[-1], 128) * jnp.dtype(item.dtype).itemsize
    return min(max(total // (1024 * 1024) + extra, 52), 60) * 1024 * 1024


def greet_some(targets):
    barrier = pltpu.get_barrier_semaphore()
    count = 0
    for here, target in targets:

        @pl.when(here)
        def _():
            pl.semaphore_signal(barrier, inc=1, device_id=target, device_id_type=MESH)

        count = count + jnp.where(here, 1, 0)
    return lambda: pl.semaphore_wait(barrier, count)


def line(tp_count):
    sp = lax.axis_index("sp")
    tp = lax.axis_index("tp")
    core = lax.rem(tp, 2)
    z = lax.div(tp, 2)
    depth = tp_count // 2
    partner = (sp, tp + 1 - 2 * core)
    return sp, core, z, depth, partner, (sp, tp + 2), (sp, tp - 2), z < depth - 1, z > 0


def moe_kernel(
    sp_count,
    tp_count,
    spare,
    heads_ref,
    residual_ref,
    norm_gain_ref,
    extra_ref,
    rank_ref,
    gate_ref,
    up_ref,
    down_ref,
    out_ref,
    own,
    token_rows,
    held,
    picked,
    rows,
    gate,
    up,
    down,
    result,
    result_spare,
    swapped,
    swapped_spare,
    summed,
    back,
    mixed,
    stage,
    up_in,
    down_in,
    usend,
    dsend,
    recv,
    ssend,
    srecv,
    fsend,
    frecv,
    wsend,
    wrecv,
    vsend,
    vrecv,
    rsend,
    rrecv,
    zsend,
    urecv,
    drecv,
    wsem,
):
    me, core, z, depth, partner, above, below, has_above, has_below = line(tp_count)
    tp = lax.axis_index("tp")
    experts = gate_ref.shape[0]
    model = gate_ref.shape[1]
    tokens, wide = own.shape
    slots = rows.shape[3]
    low = own.dtype
    middle = model // 2
    segment = middle * spare // slots
    sent = middle + segment
    quarter = model // PIECES
    hops = [slice(i * quarter, (i + 1) * quarter) for i in range(PIECES)]
    line_parts = hops[:-1] + [slice(model - quarter, wide)]
    share_of = PIECES // 2
    parts = (slice(0, middle), slice(middle, model))
    gather_parts = (slice(0, sent), slice(sent, rows.shape[4]))
    return_parts = (slice(0, sent), slice(sent, 2 * sent))

    def fold_matrix(k, count, flat):
        full, few = count * slots, count * spare
        shape = (full, few) if flat else (few, full)
        row = lax.broadcasted_iota(jnp.int32, shape, 0 if flat else 1)
        column = lax.broadcasted_iota(jnp.int32, shape, 1 if flat else 0)
        place = row & (slots - 1)
        low_bits = spare.bit_length() - 1
        owner = (row >> (slots.bit_length() - 1)) << low_bits
        here = ((place >> low_bits) == k) & (column == owner + (row & (spare - 1)))
        return jnp.where(here, 1.0, 0.0).astype(low)

    def fold(extra_rows):
        count = extra_rows.shape[0] // spare
        total = None
        for k in range(slots // spare):
            piece = extra_rows[:, k * segment : (k + 1) * segment]
            matrix = fold_matrix(k, count, True)
            term = jnp.dot(matrix, piece, preferred_element_type=jnp.float32)
            total = term if k == 0 else total + term
        return total.astype(low)

    def unfold(folded):
        count = folded.shape[0] // slots
        pieces = [
            jnp.dot(fold_matrix(k, count, False), folded, preferred_element_type=jnp.float32)
            for k in range(slots // spare)
        ]
        return jnp.concatenate(pieces, axis=1).astype(low)

    def one_hot(place, start, height, limit):
        row = lax.broadcasted_iota(jnp.int32, (height, tokens), 0)
        wanted = jnp.where(row < limit, row + start, -2)
        pieces = [
            jnp.where(rank_ref[place, source : source + 1] == wanted, 1.0, 0.0)
            for source in range(sp_count)
        ]
        return jnp.concatenate(pieces, axis=0)

    def spare_hot(place):
        full = one_hot(place, slots, slots, spare)
        matrix = fold_matrix(0, sp_count, False)
        return jnp.dot(matrix, full.astype(low), preferred_element_type=jnp.float32)

    others = [lax.rem(me + k, sp_count) for k in reversed(range(1, sp_count))]
    loads = [
        pltpu.make_async_copy(source, target, wsem.at[i])
        for i, (source, target) in enumerate(((gate_ref, gate), (up_ref, up), (down_ref, down)))
    ]
    met = greet_some(
        [(True, partner), (has_above, above), (has_below, below)]
        + [(True, (other, tp)) for other in others]
    )
    for load in loads:
        load.start()
    total = residual_ref[...].astype(jnp.float32) + heads_ref[...]
    token_rows[...] = total
    own[:, :model] = rms_scale(total, norm_gain_ref[...]).astype(low)
    own[:, model:] = extra_ref[...]
    met()

    def move(place, sems, part, target, source=None):
        source = held.at[place] if source is None else source
        return remote(
            source.at[:, line_parts[part]],
            held.at[place, :, line_parts[part]],
            sems.at[place, part],
            recv.at[place, part],
            target,
        )

    for part in range(PIECES):

        @pl.when(has_above)
        def _():
            move(z, usend, part, above, own).start()

        @pl.when(has_below)
        def _():
            move(z, dsend, part, below, own).start()

    held[z] = own[...]
    def send_to(source, target, sends, recvs, place, part, mark, arrive, device):
        return remote(
            source, target, sends.at[place, mark, part], recvs.at[place, arrive, part], device
        )

    def spread(place, part, other, arrive=None):
        arrive = me if arrive is None else arrive
        span = gather_parts[part]
        return send_to(
            picked.at[place, other, :, span],
            rows.at[place, core, arrive, :, span],
            ssend,
            srecv,
            place,
            part,
            other,
            arrive,
            (other, tp),
        )

    def share(place, part, source, own_rows=False):
        span = gather_parts[part]
        target = rows.at[place, core, source, :, span]
        start = picked.at[place, source, :, span] if own_rows else target
        return send_to(start, target, fsend, frecv, place, part, source, source, partner)

    def shared(place, part, source):
        target = rows.at[place, 1 - core, source, :, gather_parts[part]]
        return send_to(target, target, fsend, frecv, place, part, source, source, partner)

    def swap(place, part):
        return remote(
            result.at[place, 1 - core, :, :, parts[part]],
            swapped.at[place, :, :, parts[part]],
            wsend.at[place, part],
            wrecv.at[place, part],
            partner,
        )

    def swap_spare(place, part):
        return remote(
            result_spare.at[place, 1 - core, :, parts[part]],
            swapped_spare.at[place, :, parts[part]],
            vsend.at[place, part],
            vrecv.at[place, part],
            partner,
        )

    def give(place, part, other, arrive=None):
        arrive = me if arrive is None else arrive
        span = return_parts[part]
        return send_to(
            summed.at[place, other, :, span],
            back.at[place, arrive, :, span],
            rsend,
            rrecv,
            place,
            part,
            other,
            arrive,
            (other, tp),
        )

    def pass_on(place, part, arrivals, sems, target):
        return remote(
            stage.at[place, :, hops[part]],
            arrivals.at[place, :, hops[part]],
            zsend.at[place, part],
            sems.at[place, part],
            target,
        )

    def rise(place, part):
        return pass_on(place, part, up_in, urecv, above)

    def fall(place, part):
        return pass_on(place, part, down_in, drecv, below)

    def take(k, part):
        lower, upper = z - k, z + k

        @pl.when((k > 0) & (lower >= 0))
        def _():
            move(lower, usend, part, below).wait_recv()

            @pl.when(has_above)
            def _():
                move(lower, usend, part, above).start()

        @pl.when((k > 0) & (upper < depth))
        def _():
            move(upper, dsend, part, above).wait_recv()

            @pl.when(has_below)
            def _():
                move(upper, dsend, part, below).start()

    def choose(place, part):
        span = parts[part]
        base = gather_parts[part].start
        inputs = held[place, :, span]
        pick = one_hot(place, 0, slots, slots).astype(low)

        def keep(value, start):
            width = value.shape[1]
            picked[place, :, :, start : start + width] = value.astype(low).reshape(
                sp_count, slots, width
            )

        keep(jnp.dot(pick, inputs, preferred_element_type=jnp.float32), base)
        if spare:
            few = spare_hot(place).astype(low)
            extra_rows = jnp.dot(few, inputs, preferred_element_type=jnp.float32).astype(low)
            keep(fold(extra_rows), base + middle)
        if part == 1:
            tail = held[place, :, model:]
            chosen = jnp.dot(pick, tail, preferred_element_type=jnp.float32)
            if spare:
                full = one_hot(place, slots, slots, spare).astype(low)
                second = jnp.dot(full, tail, preferred_element_type=jnp.float32)
                lane = lax.broadcasted_iota(jnp.int32, chosen.shape, 1)
                chosen = jnp.where(lane < 64, chosen, second)
            keep(chosen, 2 * sent)
        for other in others:
            spread(place, part, other).start()
        share(place, part, me, True).start()
        rows[place, core, me, :, gather_parts[part]] = picked[place, me, :, gather_parts[part]]

    def relay(place, part):
        for other in others:
            spread(place, part, other, other).wait_recv()
            share(place, part, other).start()

    def compute(place):
        for part in range(2):
            for source in range(sp_count):
                shared(place, part, source).wait_recv()
        count = 2 * sp_count
        full = count * slots

        def stretch(start, width):
            return rows[place, :, :, :, start : start + width].reshape(full, width)

        inputs = []
        for part in range(2):
            x = stretch(part * sent, middle)
            if spare:
                few = unfold(stretch(part * sent + middle, segment))
                x = jnp.concatenate([x, few], axis=0)
            inputs.append(x)
        tail = stretch(2 * sent, 128)
        tails = [(tail.astype(jnp.float32), 0)]
        if spare:
            first = fold_matrix(0, count, False)
            tails.append((jnp.dot(first, tail, preferred_element_type=jnp.float32), 64))

        def scale_of(values, index):
            lane = lax.broadcasted_iota(jnp.int32, values.shape, 1)
            here = (lane == index) | (lane == index + experts * sp_count)
            return jnp.sum(jnp.where(here, values, 0.0), axis=1, keepdims=True)

        def expand(weight):
            return jnp.dot(
                inputs[0], weight[:middle], preferred_element_type=jnp.float32
            ) + jnp.dot(inputs[1], weight[middle:], preferred_element_type=jnp.float32)

        hidden = []
        for e in range(experts):
            index = me * experts + e
            scale = [scale_of(values, index + start) for values, start in tails]
            scale = jnp.concatenate(scale, axis=0) if spare else scale[0]
            gate_out = expand(gate.at[e])
            up_out = expand(up.at[e])
            hidden.append((jax.nn.silu(gate_out) * up_out * scale).astype(low))
        for part in range(2):
            span = parts[part]
            total = jnp.dot(hidden[0], down[0, :, span], preferred_element_type=jnp.float32)
            for e in range(1, experts):
                total += jnp.dot(hidden[e], down[e, :, span], preferred_element_type=jnp.float32)
            total = total.astype(low)
            result[place, :, :, :, span] = total[:full].reshape(2, sp_count, slots, middle)
            if spare:
                result_spare[place, :, :, span] = total[full:].reshape(
                    2, sp_count * spare, middle
                )
                swap_spare(place, part).start()
            swap(place, part).start()

    def settle(place, part):
        span = parts[part]
        base = return_parts[part].start
        swap(place, part).wait_recv()
        kept = result[place, core, :, :, span].astype(jnp.float32)
        both = kept + swapped[place, :, :, span].astype(jnp.float32)
        summed[place, :, :, base : base + middle] = both.astype(low)
        if spare:
            swap_spare(place, part).wait_recv()
            kept = result_spare[place, core, :, span].astype(jnp.float32)
            both = kept + swapped_spare[place, :, span].astype(jnp.float32)
            summed[place, :, :, base + middle : base + sent] = fold(both.astype(low)).reshape(
                sp_count, slots, segment
            )
        for other in others:
            give(place, part, other).start()
        back[place, me, :, base : base + sent] = summed[place, me, :, base : base + sent]

    def combine(place, part):
        span = parts[part]
        base = return_parts[part].start
        for other in others:
            give(place, part, other, other).wait_recv()

        def gathered(start, width):
            return back[place, :, :, start : start + width].reshape(sp_count * slots, width)

        total = jnp.dot(
            one_hot(place, 0, slots, slots).T.astype(low),
            gathered(base, middle),
            preferred_element_type=jnp.float32,
        )
        if spare:
            total += jnp.dot(
                spare_hot(place).T.astype(low),
                unfold(gathered(base + middle, segment)),
                preferred_element_type=jnp.float32,
            )
        mixed[place, :, span] = total

        for hop in range(part * share_of, (part + 1) * share_of):
            span = hops[hop]

            @pl.when((place > z) & (z == 0))
            def _():
                stage[place, :, span] = mixed[place, :, span].astype(low)
                rise(place, hop).start()

            @pl.when((place < z) & (z == depth - 1))
            def _():
                stage[place, :, span] = mixed[place, :, span].astype(low)
                fall(place, hop).start()

    def at(k, action):
        def one(side, unused):
            place = z + (1 - 2 * side) * k

            @pl.when((place >= 0) & (place < depth) & ((k > 0) | (side == 0)) & (k >= 0))
            def _():
                action(place)

            return unused

        lax.fori_loop(0, 2, one, 0)

    def step(t, unused):
        @pl.when(t < depth)
        def _():
            for part in range(2):
                for piece in range(part * share_of, (part + 1) * share_of):
                    take(t, piece)
                at(t, lambda place: choose(place, part))

        @pl.when(t == 1)
        def _():
            for load in loads:
                load.wait()

        for action, late in ((relay, 1), (settle, 2), (combine, 3)):
            for part in range(2):
                at(t - late, lambda place: action(place, part))
        at(t - 1, compute)
        return unused

    lax.fori_loop(0, depth + 3, step, 0)

    def hop(key, unused):
        high = key - z
        deep = 2 * depth - 2 - key - z
        for part in range(PIECES):
            span = hops[part]

            @pl.when((high > z) & (high < depth) & has_below)
            def _():
                rise(high, part).wait_recv()
                stage[high, :, span] = (
                    mixed[high, :, span] + up_in[high, :, span].astype(jnp.float32)
                ).astype(low)
                rise(high, part).start()

            @pl.when((deep >= 0) & (deep < z) & has_above)
            def _():
                fall(deep, part).wait_recv()
                stage[deep, :, span] = (
                    mixed[deep, :, span] + down_in[deep, :, span].astype(jnp.float32)
                ).astype(low)
                fall(deep, part).start()

        return unused

    lax.fori_loop(1, 2 * depth - 2, hop, 0)
    for part in range(PIECES):
        span = hops[part]
        token_rows[:, span] += mixed[z, :, span]

        @pl.when(has_below)
        def _():
            rise(z, part).wait_recv()
            token_rows[:, span] += up_in[z, :, span].astype(jnp.float32)

        @pl.when(has_above)
        def _():
            fall(z, part).wait_recv()
            token_rows[:, span] += down_in[z, :, span].astype(jnp.float32)

        out_ref[:, span] = token_rows[:, span].astype(low)

    def finish(place, unused):
        for part in range(PIECES):

            @pl.when(has_above & (place <= z))
            def _():
                move(place, usend, part, above).wait_send()

            @pl.when(has_below & (place >= z))
            def _():
                move(place, dsend, part, below).wait_send()

            @pl.when(place > z)
            def _():
                rise(place, part).wait_send()

            @pl.when(place < z)
            def _():
                fall(place, part).wait_send()

        for part in range(2):
            for other in others:
                spread(place, part, other).wait_send()
                share(place, part, other).wait_send()
                give(place, part, other).wait_send()
            share(place, part, me, True).wait_send()
            swap(place, part).wait_send()
            if spare:
                swap_spare(place, part).wait_send()
        return unused

    lax.fori_loop(0, depth, finish, 0)


def moe(
    heads,
    residual,
    norm_gain,
    extra,
    rank,
    slots,
    gate_weight,
    up_weight,
    down_weight,
    sp_count,
    tp_count,
    identity,
):
    dma = pltpu.SemaphoreType.DMA
    depth = tp_count // 2
    tokens, model = residual.shape
    wide = model + extra.shape[1]
    low = residual.dtype
    spare = slots % 8
    fits = spare in (1, 2, 4) and slots - spare in (8, 16, 32, 64)
    if fits and model // 2 * spare // (slots - spare) % 128 == 0:
        slots = slots - spare
    else:
        spare = 0
        slots = -(-slots // 8) * 8
    sent = model // 2 * (slots + spare) // slots
    anywhere = pl.BlockSpec(memory_space=pl.ANY)
    each = dma((depth, sp_count, 2))
    two = dma((depth, 2))
    fine = dma((depth, PIECES))
    block = pltpu.VMEM((depth, tokens, model), low)
    group = pltpu.VMEM((depth, sp_count, slots, model), low)
    carried = pltpu.VMEM((depth, sp_count, slots, 2 * sent), low)
    few = max(spare * sp_count, 8)
    scratch = [
        pltpu.VMEM((tokens, wide), low),
        pltpu.VMEM((tokens, model), jnp.float32),
        pltpu.VMEM((depth, tokens, wide), low),
        pltpu.VMEM((depth, sp_count, slots, 2 * sent + 128), low),
        pltpu.VMEM((depth, 2, sp_count, slots, 2 * sent + 128), low),
        pltpu.VMEM(gate_weight.shape, gate_weight.dtype),
        pltpu.VMEM(up_weight.shape, up_weight.dtype),
        pltpu.VMEM(down_weight.shape, down_weight.dtype),
        pltpu.VMEM((depth, 2, sp_count, slots, model), low),
        pltpu.VMEM((depth, 2, few, model), low),
        group,
        pltpu.VMEM((depth, few, model), low),
        carried,
        carried,
        pltpu.VMEM((depth, tokens, model), jnp.float32),
        block,
        block,
        block,
        fine,
        fine,
        fine,
        each,
        each,
        each,
        each,
        two,
        two,
        two,
        two,
        each,
        each,
        fine,
        fine,
        fine,
        dma((3,)),
    ]
    return pl.pallas_call(
        functools.partial(moe_kernel, sp_count, tp_count, spare),
        out_shape=jax.ShapeDtypeStruct((tokens, model), low),
        in_specs=[VM, VM, VM, VM, VM, anywhere, anywhere, anywhere],
        out_specs=VM,
        scratch_shapes=scratch,
        compiler_params=pltpu.CompilerParams(
            collective_id=identity, has_side_effects=True, vmem_limit_bytes=grant(scratch, 8)
        ),
    )(heads, residual, norm_gain[None, :], extra, rank, gate_weight, up_weight, down_weight)


NT = (((1,), (1,)), ((), ()))


def attend_kernel(
    rope_width,
    sp_count,
    tp_count,
    latent_ref,
    gain_ref,
    key_rope_ref,
    q_ref,
    q_rope_ref,
    cos_ref,
    sin_ref,
    wk_ref,
    wv_ref,
    wo_ref,
    out_ref,
    latent,
    queries,
    wk_raw,
    wv_raw,
    wo,
    own,
    held,
    qx,
    wk,
    wvt,
    kx,
    vt,
    tops,
    sums,
    acc,
    attention,
    partial,
    partner_in,
    stage,
    up_in,
    down_in,
    wsem,
    send,
    recv,
    fsend,
    psend,
    precv,
    zsend,
    urecv,
    drecv,
):
    me, core, z, depth, partner, above, below, has_above, has_below = line(tp_count)
    tp = lax.axis_index("tp")
    tokens, width = latent.shape
    pairs, pair_width = queries.shape[1:]
    half = tokens // 2
    low = own.dtype
    loads = [
        pltpu.make_async_copy(source, target, wsem.at[i])
        for i, (source, target) in enumerate(
            (
                (latent_ref, latent),
                (q_ref, queries),
                (wk_ref, wk_raw),
                (wv_ref, wv_raw),
                (wo_ref, wo),
            )
        )
    ]
    loads[0].start()
    met = greet_some(
        [(True, partner), (has_above, above), (has_below, below)]
        + [(True, (lax.rem(me + k, sp_count), tp)) for k in range(1, sp_count)]
    )
    mine = pl.ds(pl.multiple_of(core * half, half), half)
    other = pl.ds(pl.multiple_of((1 - core) * half, half), half)

    def outgoing(to):
        return remote(own.at[mine], held.at[me, mine], send.at[to], recv.at[me, core], (to, tp))

    def incoming(source):
        return remote(
            own.at[mine], held.at[source, mine], send.at[source], recv.at[source, core], partner
        )

    def forward(source):
        return remote(
            held.at[source, mine],
            held.at[source, mine],
            fsend.at[source],
            recv.at[source, core],
            partner,
        )

    def forwarded(source):
        return remote(
            held.at[source, other],
            held.at[source, other],
            fsend.at[source],
            recv.at[source, 1 - core],
            partner,
        )

    turn = rope_width // 2
    cosine, sine = cos_ref[...], sin_ref[...]

    def rotate(upper, lower):
        return upper * cosine - lower * sine, lower * cosine + upper * sine

    raw = key_rope_ref[...].astype(jnp.float32)
    rotated = list(rotate(raw[:turn], raw[turn:]))
    own[:, width:] = jnp.concatenate(rotated * (128 // rope_width), axis=0).T.astype(low)
    loads[0].wait()
    for load in loads[1:]:
        load.start()
    values = latent[...].astype(jnp.float32)
    inverse = lax.rsqrt(jnp.mean(values * values, axis=-1, keepdims=True) + epsilon)
    own[:, :width] = (values * inverse * gain_ref[...]).astype(low)

    met()
    for to in reversed(range(sp_count)):

        @pl.when(to > me)
        def _():
            outgoing(to).start()

    def merge(one, two):
        lane = lax.broadcasted_iota(jnp.int32, one.shape, 1)
        return jnp.where(lane < DK_A, one, two)

    for load in loads[1:4]:
        load.wait()
    gap = jnp.zeros((DK_A - rope_width, tokens), jnp.float32)
    for pair in range(pairs):
        rope = q_rope_ref[pair].astype(jnp.float32)
        first = list(rotate(rope[:turn], rope[turn:rope_width]))
        second = list(rotate(rope[rope_width : rope_width + turn], rope[rope_width + turn :]))
        turned = jnp.concatenate(second + [gap] + first + [gap], axis=0).T.astype(low)
        qx[pair, :, 128:] = queries[:, pair, :]
        query = qx[pair, :, 128:256]
        qx[pair, :, :128] = merge(query, turned)
        qx[pair, :, 128:256] = merge(turned, query)
        wk[pair] = wk_raw[:, pair, :]
        wvt[pair] = wv_raw[:, pair, :].T
    scales = [
        size ** (-0.5) * 1.4426950408889634
        for size in (DK_A + rope_width, pair_width - DK_A + rope_width)
    ]
    splits = ((slice(0, 128), slice(0, DV_A)), (slice(128, None), slice(DV_A, pair_width)))

    def ahead(index):
        @pl.when(index >= 0)
        def _():
            incoming(index).wait_recv()
            forward(index).start()

    def block(index, first):
        source = own if first else held.at[index]
        compressed = source[:, :width]
        rope = source[:, width:]
        for pair in range(pairs):
            rows = jnp.dot(compressed, wk[pair], preferred_element_type=jnp.float32).astype(low)
            kx[pair, :, :128] = merge(rows[:, :128], rope)
            kx[pair, :, 128:256] = merge(rope, rows[:, :128])
            kx[pair, :, 256:] = rows[:, 128:]
            vt[pair] = lax.dot_general(
                wvt[pair], compressed, NT, preferred_element_type=jnp.float32
            ).astype(low)
        for pair in range(pairs):
            if pair == 1 and not first:
                ahead(index - 1)
            for group, (span, part) in enumerate(splits):
                head = pair * 2 + group
                scores = lax.dot_general(
                    kx[pair, :, span], qx[pair, :, span], NT, preferred_element_type=jnp.float32
                )
                if first:
                    row = lax.broadcasted_iota(jnp.int32, (tokens, tokens), 0)
                    column = lax.broadcasted_iota(jnp.int32, (tokens, tokens), 1)
                    scores = jnp.where(row <= column, scores, floor_score)
                    top = jnp.max(scores, axis=0, keepdims=True)
                else:
                    old = tops[head]
                    top = jnp.maximum(old, jnp.max(scores, axis=0, keepdims=True))
                    factor = jnp.exp2((old - top) * scales[group])
                weights = jnp.exp2((scores - top) * scales[group])
                total = jnp.sum(weights, axis=0, keepdims=True)
                update = jnp.dot(
                    vt[pair, part], weights.astype(low), preferred_element_type=jnp.float32
                )
                tops[head] = top
                if first:
                    sums[head] = total
                    acc[pair, part] = update
                else:
                    sums[head] = sums[head] * factor + total
                    acc[pair, part] = acc[pair, part] * factor + update

    block(me, True)
    ahead(me - 1)

    def step(i, unused):
        index = me - 1 - i
        forwarded(index).wait_recv()
        block(index, False)
        return unused

    lax.fori_loop(0, me, step, 0)
    for pair in range(pairs):
        for group, (span, part) in enumerate(splits):
            acc[pair, part] = acc[pair, part] / sums[pair * 2 + group]
        attention[:, pair * pair_width : (pair + 1) * pair_width] = acc[pair].T.astype(low)

    row_count, model = out_ref.shape
    quarter = model // PIECES
    parts = [slice(i * quarter, (i + 1) * quarter) for i in range(PIECES)]

    def swap(place, part):
        return remote(
            partial.at[place * 2 + 1 - core, :, parts[part]],
            partner_in.at[place, :, parts[part]],
            psend.at[place, part],
            precv.at[place, part],
            partner,
        )

    def pass_on(place, part, arrivals, sems, target):
        return remote(
            stage.at[place, :, parts[part]],
            arrivals.at[place, :, parts[part]],
            zsend.at[place, part],
            sems.at[place, part],
            target,
        )

    def up(place, part):
        return pass_on(place, part, up_in, urecv, above)

    def down(place, part):
        return pass_on(place, part, down_in, drecv, below)

    def pair_sum(place, part):
        swap(place, part).wait_recv()
        kept = partial[place * 2 + core, :, parts[part]].astype(jnp.float32)
        return kept + partner_in[place, :, parts[part]].astype(jnp.float32)

    def project(n, unused):
        turnabout = lax.rem(n, 2)
        place = turnabout * (n // 2) + (1 - turnabout) * (depth - 1 - n // 2)
        rows = pl.ds(pl.multiple_of(place * 2 * row_count, 2 * row_count), 2 * row_count)
        inputs = attention[rows]
        for part in range(PIECES):
            mixed = jnp.dot(inputs, wo[:, parts[part]], preferred_element_type=jnp.float32)
            mixed = mixed.astype(low).reshape(2, row_count, mixed.shape[1])
            partial[pl.ds(place * 2, 2), :, parts[part]] = mixed
            swap(place, part).start()
        return unused

    loads[4].wait()
    lax.fori_loop(0, depth, project, 0)

    for j in range(depth - 1):
        high, deep = depth - 1 + z - j, j + z + 1 - depth
        for part in range(PIECES):
            span = parts[part]

            @pl.when(z <= j)
            def _():
                stage[high, :, span] = pair_sum(high, part).astype(low)

                @pl.when(has_below)
                def _():
                    up(high, part).wait_recv()
                    stage[high, :, span] = (
                        stage[high, :, span].astype(jnp.float32)
                        + up_in[high, :, span].astype(jnp.float32)
                    ).astype(low)

                up(high, part).start()

            @pl.when(deep >= 0)
            def _():
                stage[deep, :, span] = pair_sum(deep, part).astype(low)

                @pl.when(has_above)
                def _():
                    down(deep, part).wait_recv()
                    stage[deep, :, span] = (
                        stage[deep, :, span].astype(jnp.float32)
                        + down_in[deep, :, span].astype(jnp.float32)
                    ).astype(low)

                down(deep, part).start()

    for part in range(PIECES):
        span = parts[part]
        out_ref[:, span] = pair_sum(z, part)

        @pl.when(has_below)
        def _():
            up(z, part).wait_recv()
            out_ref[:, span] += up_in[z, :, span].astype(jnp.float32)

        @pl.when(has_above)
        def _():
            down(z, part).wait_recv()
            out_ref[:, span] += down_in[z, :, span].astype(jnp.float32)

    for place in range(sp_count):

        @pl.when(place < me)
        def _():
            forward(place).wait_send()

        @pl.when(place > me)
        def _():
            outgoing(place).wait_send()

    for place in range(depth):
        for part in range(PIECES):
            swap(place, part).wait_send()

            @pl.when(place > z)
            def _():
                up(place, part).wait_send()

            @pl.when(place < z)
            def _():
                down(place, part).wait_send()


def attend(
    latent,
    latent_gain,
    key_rope,
    queries,
    query_rope,
    cosine,
    sine,
    key_weight,
    value_weight,
    out_weight,
    sp_count,
    tp_count,
    identity,
):
    tokens, latent_width = latent.shape
    pairs, pair_width = queries.shape[1:]
    rope_width = key_rope.shape[1]
    model = out_weight.shape[1]
    low = latent.dtype
    row_count = tokens // tp_count
    depth = tp_count // 2
    dma = pltpu.SemaphoreType.DMA
    vmem = pltpu.VMEM
    f32 = jnp.float32
    padded = pair_width + 128
    anywhere = pl.BlockSpec(memory_space=pl.ANY)
    block = vmem((depth, row_count, model), low)
    scratch = [
        vmem(latent.shape, low),
        vmem(queries.shape, low),
        vmem(key_weight.shape, low),
        vmem(value_weight.shape, low),
        vmem(out_weight.shape, low),
        vmem((tokens, latent_width + 128), low),
        vmem((sp_count, tokens, latent_width + 128), low),
        vmem((pairs, tokens, padded), low),
        vmem((pairs, latent_width, pair_width), low),
        vmem((pairs, pair_width, latent_width), low),
        vmem((pairs, tokens, padded), low),
        vmem((pairs, pair_width, tokens), low),
        vmem((2 * pairs, 1, tokens), f32),
        vmem((2 * pairs, 1, tokens), f32),
        vmem((pairs, pair_width, tokens), f32),
        vmem((tokens, pairs * pair_width), low),
        vmem((tp_count, row_count, model), low),
        block,
        block,
        block,
        block,
        dma((5,)),
        dma((sp_count,)),
        dma((sp_count, 2)),
        dma((sp_count,)),
        dma((depth, PIECES)),
        dma((depth, PIECES)),
        dma((depth, PIECES)),
        dma((depth, PIECES)),
        dma((depth, PIECES)),
    ]
    return pl.pallas_call(
        functools.partial(attend_kernel, rope_width, sp_count, tp_count),
        out_shape=jax.ShapeDtypeStruct((row_count, model), f32),
        in_specs=[anywhere, VM, VM, anywhere, VM, VM, VM, anywhere, anywhere, anywhere],
        out_specs=VM,
        scratch_shapes=scratch,
        compiler_params=pltpu.CompilerParams(
            collective_id=identity, has_side_effects=True, vmem_limit_bytes=60 * 1024 * 1024
        ),
    )(
        latent,
        latent_gain[None, :],
        key_rope.T,
        queries,
        query_rope.transpose(1, 2, 0),
        cosine,
        sine,
        key_weight,
        value_weight,
        out_weight,
    )


def local(
    residual,
    queries,
    query_rope,
    latent,
    key_rope,
    latent_gain,
    key_weight,
    value_weight,
    out_weight,
    norm_gain,
    routes,
    group_gate,
    expert_share,
    gate_weight,
    up_weight,
    down_weight,
):
    tokens = queries.shape[0]
    pair_dev = queries.shape[1]
    sp_count = lax.axis_size("sp")
    tp_count = lax.axis_size("tp")
    row_count = tokens // tp_count
    rope_width = key_rope.shape[1]
    low = jnp.bfloat16

    first_place = lax.axis_index("sp") * tokens
    places = (first_place + jnp.arange(tokens, dtype=jnp.int32)).astype(jnp.float32)
    cosine, sine = angle_tables(places, rope_width)
    head_total = attend(
        latent,
        latent_gain,
        key_rope,
        queries,
        query_rope,
        cosine,
        sine,
        key_weight,
        value_weight,
        out_weight.reshape(-1, residual.shape[1]),
        sp_count,
        tp_count,
        0,
    )
    routes, group_gate, expert_share, head_total = lax.optimization_barrier(
        (routes, group_gate, expert_share, head_total)
    )
    experts_dev = gate_weight.shape[0]
    experts_all = experts_dev * sp_count
    top_count = routes.shape[1]
    depth = tp_count // 2
    capacity = max(2, 3 * row_count * top_count // (2 * experts_all))
    slots = experts_dev * capacity
    if experts_all // GROUPS == experts_dev == top_count:
        slots = capacity
    tp = lax.axis_index("tp")
    own = lax.dynamic_slice_in_dim(routes, tp * row_count, row_count, 0)
    route_weight = group_gate[:, None] * expert_share / jnp.sum(expert_share, axis=1, keepdims=True)
    expert_ids = jnp.arange(experts_all, dtype=jnp.int32)
    named = own[:, :, None] == expert_ids[None, None, :]
    table = jnp.sum(jnp.where(named, route_weight[:, :, None], 0.0), axis=1)
    weight_high = table.astype(low)
    weight_low = (table - weight_high.astype(jnp.float32)).astype(low)
    extra = jnp.concatenate([weight_high, weight_low], axis=1)
    extra = jnp.pad(extra, ((0, 0), (0, 64 - extra.shape[1])))
    extra = jnp.concatenate([extra, extra], axis=1)

    column = lax.dynamic_index_in_dim(
        routes.reshape(depth, 2, row_count, top_count), lax.rem(tp, 2), 1, keepdims=False
    )
    goal = column // experts_dev
    member = jnp.any(goal[:, :, :, None] == jnp.arange(sp_count, dtype=jnp.int32), axis=2)
    row = jnp.arange(row_count, dtype=jnp.int32)
    earlier = (row[:, None] > row[None, :]).astype(low)
    member = member.astype(low)
    rank = jnp.einsum("rq,zqs->zsr", earlier, member, preferred_element_type=jnp.float32)
    rank = jnp.where(jnp.swapaxes(member, 1, 2) > 0, rank.astype(jnp.int32), -1)
    return moe(
        head_total,
        residual,
        norm_gain,
        extra,
        rank,
        slots,
        gate_weight,
        up_weight,
        down_weight,
        sp_count,
        tp_count,
        3,
    )


def solution(mesh):
    return jax.shard_map(
        local,
        mesh=mesh,
        in_specs=(
            P(("sp", "tp"), None),
            P("sp", "tp", None),
            P("sp", "tp", None),
            P("sp", None),
            P("sp", None),
            P(),
            P(None, "tp", None),
            P(None, "tp", None),
            P("tp", None, None),
            P(),
            P("sp", None),
            P(("sp", "tp")),
            P(("sp", "tp"), None),
            P("sp", None, "tp"),
            P("sp", None, "tp"),
            P("sp", "tp", None),
        ),
        out_specs=P(("sp", "tp"), None),
        check_vma=False,
    )
```
